512 devices in a mesh: sp: 64 (over z, y), tp: 8 (over x, core).
Axes of the slice: x: 4, y: 4, z: 16, core: 2. Of those that a mesh axis runs over, the one named last changes fastest.
Arguments:
- tokens: bfloat16 [16384, 2048], P('sp', 'tp'), may hold values from -6 to 6
- norm_gain: float32 [2048], replicated, may hold values from 0.1 to 1.9
- glu_value: bfloat16 [2048, 2048], P('sp', 'tp'), may hold values from -0.125 to 0.125
- glu_gate: bfloat16 [2048, 2048], P('sp', 'tp'), may hold values from -0.125 to 0.125
- conv_taps: float32 [31, 2048], P(None, 'tp'), may hold values from -11 to 11
- ln_gain: float32 [2048], P('tp'), may hold values from 0.1 to 1.9
- ln_bias: float32 [2048], P('tp'), may hold values from -3 to 3
- query_weight: bfloat16 [2048, 2048], P('sp', 'tp'), may hold values from -0.125 to 0.125
- key_weight: bfloat16 [2048, 2048], P('sp', 'tp'), may hold values from -0.125 to 0.125
- value_weight: bfloat16 [2048, 2048], P('sp', 'tp'), may hold values from -0.125 to 0.125
- gate_weight: bfloat16 [2048, 32], replicated, may hold values from -0.125 to 0.125
- gate_bias: float32 [32], replicated, may hold values from -1 to 110
- log_decay_extra: float32 [16384, 16], P('sp'), may hold values from -1.3 to 0
- mem_gain: float32 [2048], P('tp'), may hold values from 0.1 to 1.9
- out_conv: bfloat16 [2048, 2048], P('tp'), may hold values from -0.125 to 0.125
- out_mem: bfloat16 [2048, 2048], P('tp'), may hold values from -0.125 to 0.125
Outputs:
- mixed: bfloat16 [16384, 2048], P(('sp', 'tp'))
The draws below stay inside these ranges and needn't reach their ends.
All inputs are finite; a program needn't handle non-finite values.
Results may differ from the reference program's by a relative error of at most 0.015.
Values may be sent and summed in bfloat16 or wider, within the bound.
A program may use at most 128 MiB of HBM per device.

```python
import math
import jax
import jax.numpy as jnp
from jax import lax

D = 2048
CONV = 2048
MEMORY_HEADS = 8
HEAD = 256
KW = 31
BLOCK = 128
MEM = 2048
SEQUENCE_TOKENS = 16384
N_TP = 8


def draw_conv_taps(key, part):
    base_key, rough_key = jax.random.split(jax.random.fold_in(key, 11))
    base = jnp.clip(jax.random.normal(base_key, (KW, CONV), jnp.float32), -4.0, 4.0)
    rising = 10.0 ** (jnp.arange(CONV, dtype=jnp.float32) / CONV)
    rough = jax.random.uniform(rough_key, (1, CONV), jnp.float32, 0.5, 1.5)
    return base * rising[None, :] * rough * KW ** (-0.5)


def draw_gate_bias(key, part):
    input_key, pick_key, fast_key, slow_key = jax.random.split(jax.random.fold_in(key, 23), 4)
    inputs = jax.random.uniform(input_key, (2, MEMORY_HEADS), jnp.float32, -1.0, 1.0)
    share = 0.5
    fast = jax.random.uniform(pick_key, (2, MEMORY_HEADS), jnp.float32) < share
    fast_bias = jax.random.uniform(fast_key, (2, MEMORY_HEADS), jnp.float32, 3.4, 4.6)
    slow_bias = math.log(SEQUENCE_TOKENS) + 1.0 + jax.random.uniform(slow_key, (2, MEMORY_HEADS), jnp.float32, 0.0, 1.0)
    forget = jnp.where(fast, fast_bias, slow_bias)
    return jnp.stack([inputs[0], forget[0], inputs[1], forget[1]]).reshape(4 * MEMORY_HEADS)


def draw_log_decay_extra(key, part):
    rate_key, place_key, loss_key = jax.random.split(jax.random.fold_in(key, 37), 3)
    blocks = SEQUENCE_TOKENS // BLOCK
    rate_low = 0.25
    rate_high = 1.0
    rates = jnp.exp(jax.random.uniform(rate_key, (blocks, 2 * MEMORY_HEADS), jnp.float32, math.log(rate_low), math.log(rate_high)))
    stable_level = jnp.repeat(rates, BLOCK, axis=0) / SEQUENCE_TOKENS
    slot_places = jax.random.randint(place_key, (3, 2 * MEMORY_HEADS), 0, SEQUENCE_TOKENS)
    loss_values = jax.random.uniform(loss_key, (3, 2 * MEMORY_HEADS), jnp.float32, 0.22, 0.41)
    token_positions = jnp.arange(SEQUENCE_TOKENS, dtype=jnp.int32)[:, None]
    spike_values = jnp.zeros((SEQUENCE_TOKENS, 2 * MEMORY_HEADS), jnp.float32)
    for spike_value in range(3):
        spike_values = spike_values + jnp.where(token_positions == slot_places[spike_value][None, :], loss_values[spike_value][None, :], 0.0)
    return -(stable_level + spike_values)


def level_of(key, extent, cuts, smallest, high):
    gain = 1.0
    for axis_at, blocks in cuts:
        steps = jax.random.uniform(jax.random.fold_in(jax.random.fold_in(key, 6), axis_at), (blocks,), jnp.float32, smallest / len(cuts), high / len(cuts))
        gain = gain * jnp.repeat(jnp.exp(steps), extent[axis_at] // blocks).reshape((-1,) + (1,) * (len(extent) - 1 - axis_at))
    return gain


def gaussian(key, extent, spread, most, cuts=(), kind=jnp.bfloat16):
    array = jax.random.normal(key, extent, jnp.float32) * spread
    if len(cuts) > 0:
        array = level_of(key, extent, cuts, -0.22, 0.18) * array
    return jnp.clip(array, min=-most, max=most).astype(kind)


def setup_inputs(seed: int = 0) -> dict:
    seeds = jax.random.split(jax.random.key(seed), 17)
    return {
        "tokens": gaussian(seeds[0], (SEQUENCE_TOKENS, D), 1.0, 6.0, ((0, 64), (1, 8))),
        "norm_gain": jnp.clip(1.0 + 0.18 * jax.random.normal(seeds[1], (D,), jnp.float32), 0.1, 1.9),
        "glu_value": gaussian(seeds[2], (D, CONV), D ** -0.5, 0.125, ((0, 64), (1, 8))),
        "glu_gate": gaussian(seeds[3], (D, CONV), D ** -0.5, 0.125, ((0, 64), (1, 8))),
        "conv_taps": draw_conv_taps(jax.random.fold_in(seeds[16], 71), 0),
        "ln_gain": jnp.clip(1.0 + 0.18 * jax.random.normal(seeds[5], (CONV,), jnp.float32), 0.1, 1.9),
        "ln_bias": gaussian(seeds[6], (CONV,), 0.5, 3.0, ((0, 8),), jnp.float32),
        "query_weight": gaussian(seeds[7], (D, MEM), D ** -0.5, 0.125, ((0, 64), (1, 8))),
        "key_weight": gaussian(seeds[8], (D, MEM), D ** -0.5, 0.125, ((0, 64), (1, 8))),
        "value_weight": gaussian(seeds[9], (D, MEM), D ** -0.5, 0.125, ((0, 64), (1, 8))),
        "gate_weight": gaussian(seeds[10], (D, 4 * MEMORY_HEADS), D ** -0.5, 0.125),
        "gate_bias": draw_gate_bias(jax.random.fold_in(seeds[16], 71), 0),
        "log_decay_extra": draw_log_decay_extra(jax.random.fold_in(seeds[16], 71), 0),
        "mem_gain": jnp.clip(1.0 + 0.18 * jax.random.normal(seeds[13], (MEM,), jnp.float32), 0.1, 1.9),
        "out_conv": gaussian(seeds[14], (CONV, D), CONV ** -0.5, 0.125, ((0, 8),)),
        "out_mem": gaussian(seeds[15], (MEM, D), MEM ** -0.5, 0.125, ((0, 8),)),
    }


EPS = 1e-06
LOW_START = -1e+30
PRECISE = lax.Precision.HIGHEST

def block_step(carried_state, block_data):
    state_mat, state_vec, stabilizer = carried_state
    queries, key_rows, value_rows, input_gate, log_forget = block_data
    key_scale = HEAD ** (-0.5)
    length = log_forget.shape[-1]
    causal = jnp.tril(jnp.ones((length, length), dtype=bool))
    decay_sum = jnp.cumsum(log_forget, axis=-1)
    log_weight = jnp.where(causal, decay_sum[:, :, None] - decay_sum[:, None, :] + input_gate[:, None, :], -jnp.inf)
    carried = decay_sum + stabilizer[:, None]
    running = jnp.maximum(carried, lax.optimization_barrier(jnp.max(log_weight, axis=-1)))
    inner_weight = jnp.exp(log_weight - running[:, :, None])
    carry_weight = jnp.exp(carried - running)
    raw_scores = jnp.einsum('htd,hsd->hts', queries, key_rows, preferred_element_type=jnp.float32)
    scores = raw_scores * key_scale * inner_weight
    query_wide = queries.astype(jnp.float32)
    numerator = carry_weight[:, :, None] * jnp.einsum('htd,hde->hte', query_wide, state_mat, precision=PRECISE)
    numerator = numerator + jnp.einsum('hts,hse->hte', scores.astype(jnp.bfloat16), value_rows, preferred_element_type=jnp.float32)
    denominator = carry_weight * jnp.einsum('htd,hd->ht', query_wide, state_vec, precision=PRECISE) + lax.optimization_barrier(jnp.sum(scores, axis=-1))
    to_end = decay_sum[:, -1:] - decay_sum + input_gate
    carried_end = decay_sum[:, -1] + stabilizer
    new_stabilizer = jnp.maximum(carried_end, lax.optimization_barrier(jnp.max(to_end, axis=-1)))
    end_weight = jnp.exp(to_end - new_stabilizer[:, None]) * key_scale
    keep_weight = jnp.exp(carried_end - new_stabilizer)
    weighted = key_rows.astype(jnp.float32) * end_weight[:, :, None]
    new_mat = keep_weight[:, None, None] * state_mat + jnp.einsum('hsd,hse->hde', weighted.astype(jnp.bfloat16), value_rows, preferred_element_type=jnp.float32)
    new_vec = keep_weight[:, None] * state_vec + lax.optimization_barrier(jnp.sum(weighted, axis=1))
    return ((new_mat, new_vec, new_stabilizer), (numerator, denominator, running, decay_sum))

def one_direction(queries, key_proj, value_proj, input_gate, log_forget):
    count = SEQUENCE_TOKENS // BLOCK

    def heads_first(tensor):
        return jnp.transpose(tensor.reshape(BLOCK, MEMORY_HEADS, HEAD), (1, 0, 2))

    def step(carried_state, block_data):
        query_blk, key_blk, value_blk, input_blk, forget_blk = block_data
        new_state, results = block_step(carried_state, (heads_first(query_blk), heads_first(key_blk), heads_first(value_blk), input_blk.T, forget_blk.T))
        numerator, denominator, running, _ = results
        return (new_state, numerator / jnp.maximum(jnp.abs(denominator), jnp.exp(-running))[:, :, None])
    start = (jnp.zeros((MEMORY_HEADS, HEAD, HEAD), jnp.float32), jnp.zeros((MEMORY_HEADS, HEAD), jnp.float32), jnp.full((MEMORY_HEADS,), LOW_START, jnp.float32))
    inputs = (queries.reshape(count, BLOCK, MEM), key_proj.reshape(count, BLOCK, MEM), value_proj.reshape(count, BLOCK, MEM), input_gate.reshape(count, BLOCK, MEMORY_HEADS), log_forget.reshape(count, BLOCK, MEMORY_HEADS))
    _, outputs = lax.scan(step, start, inputs)
    return jnp.transpose(outputs, (0, 2, 1, 3)).reshape(SEQUENCE_TOKENS, MEMORY_HEADS, HEAD)

def reference(tokens, norm_gain, glu_value, glu_gate, conv_taps, ln_gain, ln_bias, query_weight, key_weight, value_weight, gate_weight, gate_bias, log_decay_extra, mem_gain, out_conv, out_mem):
    wide = tokens.astype(jnp.float32)
    normed = (wide * lax.rsqrt(lax.optimization_barrier(jnp.mean(wide * wide, axis=-1, keepdims=True)) + EPS) * norm_gain).astype(jnp.bfloat16)
    value_sum = jnp.dot(normed, glu_value, preferred_element_type=jnp.float32)
    gate_sum = jnp.dot(normed, glu_gate, preferred_element_type=jnp.float32)
    glu = (value_sum * jax.nn.sigmoid(gate_sum)).astype(jnp.bfloat16)
    reach = KW // 2
    padded = jnp.pad(glu.astype(jnp.float32), ((reach, reach), (0, 0)))
    conv = jnp.zeros((SEQUENCE_TOKENS, CONV), jnp.float32)
    for offset in range(KW):
        conv = conv + conv_taps[offset] * padded[offset:offset + SEQUENCE_TOKENS]
    chan_mean = lax.optimization_barrier(jnp.mean(conv, axis=-1, keepdims=True))
    chan_var = lax.optimization_barrier(jnp.mean(conv * conv, axis=-1, keepdims=True)) - chan_mean * chan_mean
    normal = (conv - chan_mean) * lax.rsqrt(chan_var + EPS) * ln_gain + ln_bias
    act = (normal * jax.nn.sigmoid(normal)).astype(jnp.bfloat16)
    queries = jnp.dot(normed, query_weight, preferred_element_type=jnp.float32).astype(jnp.bfloat16)
    key_proj = jnp.dot(normed, key_weight, preferred_element_type=jnp.float32).astype(jnp.bfloat16)
    value_proj = jnp.dot(normed, value_weight, preferred_element_type=jnp.float32).astype(jnp.bfloat16)
    gates = (jnp.dot(normed, gate_weight, preferred_element_type=jnp.float32) + gate_bias).reshape(SEQUENCE_TOKENS, 4, MEMORY_HEADS)
    extra = log_decay_extra.reshape(SEQUENCE_TOKENS, 2, MEMORY_HEADS)
    forget_fwd = jax.nn.log_sigmoid(gates[:, 1]) + extra[:, 0]
    forget_bwd = jax.nn.log_sigmoid(gates[:, 3]) + extra[:, 1]
    forward_out = one_direction(queries, key_proj, value_proj, gates[:, 0], forget_fwd)
    backward_out = jnp.flip(one_direction(jnp.flip(queries, 0), jnp.flip(key_proj, 0), jnp.flip(value_proj, 0), jnp.flip(gates[:, 2], 0), jnp.flip(forget_bwd, 0)), 0)
    summed = forward_out + backward_out
    head_norm = summed * lax.rsqrt(lax.optimization_barrier(jnp.mean(summed * summed, axis=-1, keepdims=True)) + EPS)
    memory = (head_norm * mem_gain.reshape(MEMORY_HEADS, HEAD)).reshape(SEQUENCE_TOKENS, MEM).astype(jnp.bfloat16)
    conv_group = CONV // N_TP
    mem_group = MEM // N_TP
    total = jnp.zeros((SEQUENCE_TOKENS, D), jnp.float32)
    for channel_group in range(N_TP):
        conv_cols = act[:, channel_group * conv_group:(channel_group + 1) * conv_group]
        mem_cols = memory[:, channel_group * mem_group:(channel_group + 1) * mem_group]
        partial_sum = jnp.dot(conv_cols, out_conv[channel_group * conv_group:(channel_group + 1) * conv_group], preferred_element_type=jnp.float32)
        partial_sum = partial_sum + jnp.dot(mem_cols, out_mem[channel_group * mem_group:(channel_group + 1) * mem_group], preferred_element_type=jnp.float32)
        total = total + lax.optimization_barrier(partial_sum.astype(jnp.bfloat16)).astype(jnp.float32)
    return total.astype(jnp.bfloat16)
```

```python
import functools

import jax
import jax.numpy as jnp
from jax import lax
from jax.experimental import pallas as pl
from jax.experimental.pallas import tpu as pltpu
from jax.sharding import Mesh
from jax.sharding import PartitionSpec as P

MESH = pl.DeviceIdType.MESH
NZ, NY, NX = 16, 4, 4
ROWS = 32
TOKENS = 256
D = 2048


def ring(name, count):
    me = lax.axis_index(name)

    def at(step):
        return lax.rem(me + (step % count), count)

    return at


def gather_project(
    tok, wv, wg, wq, wk, wl, gain, gate_w, gate_b,
    glu_o, q_o, k_o, v_o, gates_o,
    wa, wb, rows_in, normed, own,
    az_s, az_r, ay_s, ay_r, by_s, by_r, bz_s, bz_r, tx_s, tx_r, td_s, td_r,
):
    zat, yat, xat = ring("z", NZ), ring("y", NY), ring("x", NX)
    core = lax.axis_index("c")
    other = 1 - core

    def up_z(ref_s, ref_r, src, dst, way):
        return pltpu.make_async_remote_copy(src, dst, ref_s, ref_r, device_id={"z": zat(way)}, device_id_type=MESH)

    def up_y(ref_s, ref_r, src, dst, way):
        return pltpu.make_async_remote_copy(src, dst, ref_s, ref_r, device_id={"y": yat(way)}, device_id_type=MESH)

    def up_x(ref_s, ref_r, src, dst, way):
        return pltpu.make_async_remote_copy(src, dst, ref_s, ref_r, device_id={"x": xat(way)}, device_id_type=MESH)

    def across(ref_s, ref_r, src, dst):
        return pltpu.make_async_remote_copy(src, dst, ref_s, ref_r, device_id={"c": other}, device_id_type=MESH)

    def row_at(dz, dy):
        return pl.multiple_of((zat(dz) * NY + yat(dy)) * ROWS, ROWS)

    sent = []

    def go(copy):
        copy.start()
        sent.append(copy)
        return copy

    mine = row_at(0, 0)
    a_own = [wv, wg, wq]
    b_own = [wk, wl]
    loads = []
    for n, w in enumerate(a_own):
        loads.append(pltpu.make_async_copy(w, wa.at[pl.ds(mine, ROWS), pl.ds(256 * n, 256)], own.at[n]))
    for n, w in enumerate(b_own):
        loads.append(pltpu.make_async_copy(w, wb.at[pl.ds(mine, ROWS), pl.ds(256 * n, 256)], own.at[3 + n]))
    tp_own = xat(0) * 2 + core
    loads.append(pltpu.make_async_copy(tok, rows_in.at[tp_own], own.at[5]))
    for copy in loads:
        copy.start()

    barrier = pltpu.get_barrier_semaphore()
    for dev in ({"z": zat(1)}, {"z": zat(-1)}, {"y": yat(1)}, {"y": yat(-1)}, {"x": xat(1)}, {"x": xat(-1)}, {"c": other}):
        pl.semaphore_signal(barrier, inc=1, device_id=dev, device_id_type=MESH)
    pl.semaphore_wait(barrier, 7)

    def a_block(dz, dy, lo=0, size=ROWS):
        return wa.at[pl.ds(pl.multiple_of(row_at(dz, dy) + lo, 16), size), :]

    def b_block(dz, dy, lo=0, size=ROWS):
        return wb.at[pl.ds(pl.multiple_of(row_at(dz, dy) + lo, 16), size), :]

    def b_group(dz, lo=0, size=ROWS * NY):
        return wb.at[pl.ds(pl.multiple_of(zat(dz) * (ROWS * NY) + lo, 64), size), :]

    def send_az(way, s):
        sign = 1 if way == 0 else -1
        dz = -sign * (s - 1)
        if s < 8:
            block = a_block(dz, 0)
        else:
            block = a_block(dz, 0, 16 * way, 16)
        return go(up_z(az_s.at[way, s - 1], az_r.at[way, s - 1], block, block, sign))

    def send_bz(way, s):
        sign = 1 if way == 0 else -1
        dz = -sign * (s - 1)
        if s < 8:
            block = b_group(dz)
        else:
            block = b_group(dz, 64 * way, 64)
        return go(up_z(bz_s.at[way, s - 1], bz_r.at[way, s - 1], block, block, sign))

    def y_first(n, dz):
        block = a_block(dz, 0)
        return [go(up_y(ay_s.at[n, w], ay_r.at[n, w], block, block, 1 - 2 * w)) for w in range(2)]

    def y_second(n, dz, first):
        second = []
        for w in range(2):
            first[w].wait_recv()
            sign = 1 - 2 * w
            block = a_block(dz, -sign, 16 * w, 16)
            second.append(go(up_y(ay_s.at[n, 2 + w], ay_r.at[n, 2 + w], block, block, sign)))
        return second

    for copy in loads[:3]:
        copy.wait()
    az = [send_az(0, 1), send_az(1, 1)]
    for copy in loads[3:5]:
        copy.wait()
    by1 = []
    for w in range(2):
        block = b_block(0, 0)
        by1.append(go(up_y(by_s.at[w], by_r.at[w], block, block, 1 - 2 * w)))
    loads[5].wait()
    tx1 = []
    for w in range(2):
        block = rows_in.at[tp_own]
        tx1.append(go(up_x(tx_s.at[w], tx_r.at[w], block, block, 1 - 2 * w)))
    td = [go(across(td_s.at[0], td_r.at[0], rows_in.at[tp_own], rows_in.at[tp_own]))]
    ay_next = [(0, 0, y_first(0, 0))]

    by2 = []
    for w in range(2):
        by1[w].wait_recv()
        sign = 1 - 2 * w
        block = b_block(0, -sign, 16 * w, 16)
        by2.append(go(up_y(by_s.at[2 + w], by_r.at[2 + w], block, block, sign)))
    tx2 = []
    for w in range(2):
        tx1[w].wait_recv()
        sign = 1 - 2 * w
        slot = xat(-sign) * 2 + core
        half = rows_in.at[slot, pl.ds(128 * w, 128)]
        tx2.append(go(up_x(tx_s.at[2 + w], tx_r.at[2 + w], half, half, sign)))
        td.append(go(across(td_s.at[1 + w], td_r.at[1 + w], rows_in.at[slot], rows_in.at[slot])))
    for copy in by2:
        copy.wait_recv()
    bz = [send_bz(0, 1), send_bz(1, 1)]

    ay_last = []
    for s in range(1, 9):
        fresh = []
        for w in range(2):
            sign = 1 if w == 0 else -1
            az[w].wait_recv()
            if s < 8:
                az[w] = send_az(w, s + 1)
                n = s if w == 0 else 7 + s
                fresh.append((n, -sign * s, y_first(n, -sign * s)))
        if s == 8:
            fresh.append((15, 8, y_first(15, 8)))
        for w in range(2):
            bz[w].wait_recv()
            if s < 8:
                bz[w] = send_bz(w, s + 1)
        for n, dz, first in ay_next:
            ay_last.extend(y_second(n, dz, first))
        ay_next = fresh
        if s == 1:
            slot = xat(2) * 2 + core
            for w in range(2):
                tx2[w].wait_recv()
                half = rows_in.at[slot, pl.ds(128 * w, 128)]
                td.append(go(across(td_s.at[3 + w], td_r.at[3 + w], half, half)))
        if s == 2:
            for copy in td:
                copy.wait_recv()
            square = jnp.zeros((TOKENS, 256), jnp.float32)
            for b in range(8):
                wide = rows_in[b].astype(jnp.float32)
                square = square + wide * wide
            scale = lax.rsqrt(jnp.sum(square, axis=1, keepdims=True) / D + 1e-6)
            for b in range(8):
                cols = slice(256 * b, 256 * b + 256)
                normed[:, cols] = (rows_in[b].astype(jnp.float32) * scale * gain[:, cols]).astype(jnp.bfloat16)
            gates_o[...] = jnp.dot(normed[...], gate_w[...], preferred_element_type=jnp.float32) + gate_b[...]
    for n, dz, first in ay_next:
        ay_last.extend(y_second(n, dz, first))
    k_o[...] = jnp.dot(normed[...], wb[:, 0:256], preferred_element_type=jnp.float32).astype(jnp.bfloat16)
    v_o[...] = jnp.dot(normed[...], wb[:, 256:512], preferred_element_type=jnp.float32).astype(jnp.bfloat16)
    for copy in ay_last:
        copy.wait_recv()
    value = jnp.dot(normed[...], wa[:, 0:256], preferred_element_type=jnp.float32)
    gate = jnp.dot(normed[...], wa[:, 256:512], preferred_element_type=jnp.float32)
    glu_o[...] = (value * jax.nn.sigmoid(gate)).astype(jnp.bfloat16)
    q_o[...] = jnp.dot(normed[...], wa[:, 512:768], preferred_element_type=jnp.float32).astype(jnp.bfloat16)
    for copy in sent:
        copy.wait_send()


def projected(tokens, weights, norm_gain, gate_weight, gate_bias):
    vmem = pl.BlockSpec(memory_space=pltpu.VMEM)
    hbm = pl.BlockSpec(memory_space=pl.ANY)
    bf = jnp.bfloat16
    dma = pltpu.SemaphoreType.DMA
    return pl.pallas_call(
        gather_project,
        out_shape=[jax.ShapeDtypeStruct((TOKENS, 256), bf)] * 4 + [jax.ShapeDtypeStruct((TOKENS, 32), jnp.float32)],
        in_specs=[hbm] * 6 + [vmem] * 3,
        out_specs=[vmem] * 5,
        scratch_shapes=[
            pltpu.VMEM((D, 768), bf),
            pltpu.VMEM((D, 512), bf),
            pltpu.VMEM((8, TOKENS, 256), bf),
            pltpu.VMEM((TOKENS, D), bf),
            dma((6,)),
            dma((2, 8)), dma((2, 8)),
            dma((16, 4)), dma((16, 4)),
            dma((4,)), dma((4,)),
            dma((2, 8)), dma((2, 8)),
            dma((4,)), dma((4,)),
            dma((5,)), dma((5,)),
        ],
        compiler_params=pltpu.CompilerParams(collective_id=0, has_side_effects=True, vmem_limit_bytes=40 * 1024 * 1024),
        name="gather_project",
    )(tokens, *weights, norm_gain.reshape(1, D), gate_weight, gate_bias.reshape(1, 32))

CONV = 2048
MEMORY_HEADS = 8
HEAD = 256
KW = 31
BLOCK = 128
SP = ("z", "y")
SP_TP = ("z", "y", "x", "c")
TP = ("x", "c")


EPS = 1e-06
LOW_START = -1e30
PRECISE = lax.Precision.HIGHEST


def sent_to_all(array, axis):
    copies = jnp.broadcast_to(array, (lax.axis_size(axis), *array.shape))
    return lax.all_to_all(copies, axis, split_axis=0, concat_axis=0, tiled=True)


def joined_along(blocks, dim):
    shape = list(blocks.shape[1:])
    shape[dim] *= blocks.shape[0]
    return jnp.moveaxis(blocks, 0, dim).reshape(shape)


def collect(array, axis, dim):
    blocks = sent_to_all(array, axis)
    return joined_along(blocks, dim)


def extended(cells, sides, width):
    for axis, dim in sides:
        count = lax.axis_size(axis)
        ends = count - 1
        head = lax.slice_in_dim(cells, 0, width, axis=dim)
        tail = lax.slice_in_dim(cells, cells.shape[dim] - width, cells.shape[dim], axis=dim)
        cells = jnp.concatenate(
            [
                lax.ppermute(tail, axis, [(i, (i + 1) % count) for i in range(ends)]),
                cells,
                lax.ppermute(head, axis, [((i + 1) % count, i) for i in range(ends)]),
            ],
            axis=dim,
        )
    return cells


def of_everyone(array, axis):
    return sent_to_all(array, axis).sum(axis=0)


def together(arrays, axis):
    ends = [0]
    for a in arrays:
        ends.append(ends[-1] + a.size)
    total = of_everyone(jnp.concatenate([a.ravel() for a in arrays]), axis)
    return tuple((total[b:e].reshape(a.shape) for a, b, e in zip(arrays, ends, ends[1:])))


def nothing_yet(array, identity):
    return jax.tree.map(
        lambda a, e: jnp.broadcast_to(jnp.asarray(e, a.dtype), a.shape), array, identity
    )


def prefix_by_axis(array, axes, combine, identity):
    before = start = nothing_yet(array, identity)
    total = array
    for axis in reversed(axes):
        length, place = (lax.axis_size(axis), lax.axis_index(axis))
        pieces = jax.tree.map(lambda part: lax.all_gather(part, axis), total)
        inside, total = (start, start)
        for k in range(length):
            passed = k < place
            total = combine(total, jax.tree.map(lambda part: part[k], pieces))
            inside = jax.tree.map(lambda new, old: jnp.where(passed, new, old), total, inside)
        before = combine(inside, before)
    return before


def gathered_once(array, axis):
    leaves = jax.tree.leaves(array)
    order = sorted(range(len(leaves)), key=lambda k: -leaves[k].size)
    width = (1, *leaves[order[0]].shape)[-1]
    lines = [
        jnp.pad(leaves[k].reshape(-1), (0, -leaves[k].size % width)).reshape(-1, width)
        for k in order
    ]
    both, at, found = (lax.all_gather(jnp.concatenate(lines), axis), 0, {})
    for k, line in zip(order, lines):
        section = both[:, at : at + len(line)].reshape(len(both), -1)
        found[k] = section[:, : leaves[k].size].reshape(-1, *leaves[k].shape)
        at += len(line)
    numbers = iter(range(len(leaves)))
    return jax.tree.map(lambda _: found[next(numbers)], array)


def entering(array, axes, combine, identity):
    before = start = nothing_yet(array, identity)
    total = array
    for axis in reversed(axes):
        length, place = (lax.axis_size(axis), lax.axis_index(axis))
        pieces = gathered_once(total, axis)
        inside, total = (start, start)
        for k in reversed(range(length)):
            passed = k > place
            total = combine(total, jax.tree.map(lambda part: part[k], pieces))
            inside = jax.tree.map(lambda new, old: jnp.where(passed, new, old), total, inside)
        before = combine(inside, before)
    return before


def sent_together(arrays, axis, dim, along):
    widths = [a.shape[along] for a in arrays]
    both = jnp.concatenate(arrays, axis=along)
    filled = lax.all_gather(both, axis, axis=dim, tiled=True)
    return tuple(jnp.split(filled, [sum(widths[:k]) for k in range(1, len(widths))], axis=along))


def split_up(array, dim, length):
    shape = array.shape
    blocks = array.reshape(*shape[:dim], length, shape[dim] // length, *shape[dim + 1 :])
    return jnp.moveaxis(blocks, dim, 0)


def sent_and_summed(array, axis, dim):
    length = lax.axis_size(axis)
    blocks = lax.all_to_all(split_up(array, dim, length), axis, 0, 0, tiled=True)
    return jnp.sum(blocks.astype(jnp.float32), axis=0)


def block_step(carried_state, block_data):
    state_mat, state_vec, stabilizer = carried_state
    queries, key_rows, value_rows, input_gate, log_forget = block_data
    key_scale = HEAD ** (-0.5)
    length = log_forget.shape[-1]
    causal = jnp.tril(jnp.ones((length, length), dtype=bool))
    decay_sum = jnp.cumsum(log_forget, axis=-1)
    log_weight = jnp.where(
        causal, decay_sum[:, :, None] - decay_sum[:, None, :] + input_gate[:, None, :], -jnp.inf
    )
    carried = decay_sum + stabilizer[:, None]
    running = jnp.maximum(carried, jnp.max(log_weight, axis=-1))
    inner_weight = jnp.exp(log_weight - running[:, :, None])
    carry_weight = jnp.exp(carried - running)
    raw_scores = jnp.einsum("htd,hsd->hts", queries, key_rows, preferred_element_type=jnp.float32)
    scores = raw_scores * key_scale * inner_weight
    query_wide = queries.astype(jnp.float32)
    numerator = carry_weight[:, :, None] * jnp.einsum(
        "htd,hde->hte", query_wide, state_mat, precision=PRECISE
    )
    numerator = numerator + jnp.einsum(
        "hts,hse->hte", scores.astype(jnp.bfloat16), value_rows, preferred_element_type=jnp.float32
    )
    denominator = carry_weight * jnp.einsum(
        "htd,hd->ht", query_wide, state_vec, precision=PRECISE
    ) + jnp.sum(scores, axis=-1)
    to_end = decay_sum[:, -1:] - decay_sum + input_gate
    carried_end = decay_sum[:, -1] + stabilizer
    new_stabilizer = jnp.maximum(carried_end, jnp.max(to_end, axis=-1))
    end_weight = jnp.exp(to_end - new_stabilizer[:, None]) * key_scale
    keep_weight = jnp.exp(carried_end - new_stabilizer)
    weighted = key_rows.astype(jnp.float32) * end_weight[:, :, None]
    new_mat = keep_weight[:, None, None] * state_mat + jnp.einsum(
        "hsd,hse->hde",
        weighted.astype(jnp.bfloat16),
        value_rows,
        preferred_element_type=jnp.float32,
    )
    new_vec = keep_weight[:, None] * state_vec + jnp.sum(weighted, axis=1)
    return ((new_mat, new_vec, new_stabilizer), (numerator, denominator, running, decay_sum))


def local_pass(queries, key_rows, value_rows, input_gate, log_forget):
    head_count, length, head_width = queries.shape
    count = length // BLOCK

    def blocked(tensor):
        return jnp.moveaxis(tensor.reshape((head_count, count, BLOCK) + tensor.shape[2:]), 1, 0)

    def unblocked(tensor):
        return jnp.moveaxis(tensor, 0, 1).reshape((head_count, length) + tensor.shape[3:])

    start = (
        jnp.zeros((head_count, head_width, head_width), jnp.float32),
        jnp.zeros((head_count, head_width), jnp.float32),
        jnp.full((head_count,), LOW_START, jnp.float32),
    )
    final, outputs = lax.scan(
        block_step,
        start,
        (
            blocked(queries),
            blocked(key_rows),
            blocked(value_rows),
            blocked(input_gate),
            blocked(log_forget),
        ),
    )
    numerator, denominator, running, decay_sum = outputs
    totals = decay_sum[:, :, -1]
    offsets = jnp.cumsum(totals, axis=0) - totals
    decay_sum = decay_sum + offsets[:, :, None]
    summary = (offsets[-1] + totals[-1], final[0], final[1], final[2])
    return (
        unblocked(numerator),
        unblocked(denominator),
        unblocked(running),
        unblocked(decay_sum),
        summary,
    )


def compose(earlier, later):
    early_decay, early_mat, early_vec, early_level = earlier
    late_decay, late_mat, late_vec, late_level = later
    stabilizer = jnp.maximum(early_level + late_decay, late_level)
    early_weight = jnp.exp(early_level + late_decay - stabilizer)
    late_weight = jnp.exp(late_level - stabilizer)
    return (
        early_decay + late_decay,
        early_weight[:, None, None] * early_mat + late_weight[:, None, None] * late_mat,
        early_weight[:, None] * early_vec + late_weight[:, None] * late_vec,
        stabilizer,
    )


def finish(queries, numerator, denominator, running, decay_sum, incoming):
    in_mat, in_vec, in_level = (incoming[1], incoming[2], incoming[3])
    query_wide = queries.astype(jnp.float32)
    carried = decay_sum + in_level[:, None]
    stabilizer = jnp.maximum(running, carried)
    local_weight = jnp.exp(running - stabilizer)
    carry_weight = jnp.exp(carried - stabilizer)
    numerator = local_weight[:, :, None] * numerator
    numerator = numerator + carry_weight[:, :, None] * jnp.einsum(
        "htd,hde->hte", query_wide, in_mat, precision=PRECISE
    )
    denominator = local_weight * denominator + carry_weight * jnp.einsum(
        "htd,hd->ht", query_wide, in_vec, precision=PRECISE
    )
    return numerator / jnp.maximum(jnp.abs(denominator), jnp.exp(-stabilizer))[:, :, None]


def shards(
    tokens,
    norm_gain,
    glu_value,
    glu_gate,
    conv_taps,
    ln_gain,
    ln_bias,
    query_weight,
    key_weight,
    value_weight,
    gate_weight,
    gate_bias,
    log_decay_extra,
    mem_gain,
    out_conv,
    out_mem,
):
    glu, *projected_rows, gate_sums = projected(
        tokens, (glu_value, glu_gate, query_weight, key_weight, value_weight), norm_gain, gate_weight, gate_bias
    )
    row_count = glu.shape[0]
    head_count = mem_gain.shape[0] // HEAD
    first_head = lax.axis_index(TP) * head_count
    gate_all = gate_sums.reshape(row_count, 4, MEMORY_HEADS)
    own_gates = lax.dynamic_slice_in_dim(gate_all, first_head, head_count, 2)
    own_extra = lax.dynamic_slice_in_dim(
        log_decay_extra.reshape(row_count, 2, MEMORY_HEADS), first_head, head_count, 2
    )

    def memory_branch(query_proj, key_proj, value_proj):

        def head_major(tensor):
            return jnp.transpose(tensor.reshape(row_count, head_count, HEAD), (1, 0, 2))

        queries = head_major(query_proj)
        key_rows = head_major(key_proj)
        value_rows = head_major(value_proj)
        input_fwd = own_gates[:, 0, :].T
        forget_fwd = (jax.nn.log_sigmoid(own_gates[:, 1, :]) + own_extra[:, 0, :]).T
        input_bwd = own_gates[:, 2, :].T
        forget_bwd = (jax.nn.log_sigmoid(own_gates[:, 3, :]) + own_extra[:, 1, :]).T
        identity = (
            jnp.zeros((head_count,), jnp.float32),
            jnp.zeros((head_count, HEAD, HEAD), jnp.float32),
            jnp.zeros((head_count, HEAD), jnp.float32),
            jnp.full((head_count,), LOW_START, jnp.float32),
        )
        numerator, denominator, running, decay_sum, summary = local_pass(
            queries, key_rows, value_rows, input_fwd, forget_fwd
        )
        incoming = prefix_by_axis(summary, SP, compose, identity)
        forward_out = finish(queries, numerator, denominator, running, decay_sum, incoming)
        back_queries = jnp.flip(queries, 1)
        numerator, denominator, running, decay_sum, summary = local_pass(
            back_queries,
            jnp.flip(key_rows, 1),
            jnp.flip(value_rows, 1),
            jnp.flip(input_bwd, 1),
            jnp.flip(forget_bwd, 1),
        )
        incoming = entering(summary, SP, compose, identity)
        backward_out = jnp.flip(
            finish(back_queries, numerator, denominator, running, decay_sum, incoming), 1
        )
        summed = forward_out + backward_out
        head_norm = summed * lax.rsqrt(jnp.mean(summed * summed, axis=-1, keepdims=True) + EPS)
        head_norm = head_norm * mem_gain.reshape(head_count, HEAD)[:, None, :]
        return (
            jnp.transpose(head_norm, (1, 0, 2))
            .reshape(row_count, head_count * HEAD)
            .astype(jnp.bfloat16)
        )

    reach = KW // 2
    padded = extended(glu, ((SP, 0),), reach).astype(jnp.float32)
    conv = jnp.zeros(glu.shape, jnp.float32)
    for offset in range(KW):
        conv = conv + conv_taps[offset] * padded[offset : offset + row_count]
    chan_sums = jnp.sum(conv, axis=-1)
    chan_squares = jnp.sum(conv * conv, axis=-1)
    chan_sums, chan_squares = together((chan_sums, chan_squares), TP)
    chan_mean = chan_sums / CONV
    chan_var = chan_squares / CONV - chan_mean * chan_mean
    normal = (conv - chan_mean[:, None]) * lax.rsqrt(chan_var + EPS)[:, None] * ln_gain + ln_bias
    act = (normal * jax.nn.sigmoid(normal)).astype(jnp.bfloat16)
    memory = memory_branch(*projected_rows)
    result = jnp.dot(act, out_conv, preferred_element_type=jnp.float32)
    mixed = sent_and_summed(
        (result + jnp.dot(memory, out_mem, preferred_element_type=jnp.float32)).astype(
            jnp.bfloat16
        ),
        TP,
        0,
    )
    return mixed.astype(jnp.bfloat16)


def solution(mesh):
    split = Mesh(mesh.devices.reshape(16, 4, 4, 2), ("z", "y", "x", "c"))
    placed = (
        P(SP, TP),
        P(),
        P(SP, TP),
        P(SP, TP),
        P(None, TP),
        P(TP),
        P(TP),
        P(SP, TP),
        P(SP, TP),
        P(SP, TP),
        P(),
        P(),
        P(SP, None),
        P(TP),
        P(TP, None),
        P(TP, None),
    )
    return jax.shard_map(
        shards, mesh=split, in_specs=placed, out_specs=P(SP_TP, None), check_vma=False
    )
```

```python
import functools

import jax
import jax.numpy as jnp
from jax import lax
from jax.experimental import pallas as pl
from jax.experimental.pallas import tpu as pltpu
from jax.sharding import Mesh
from jax.sharding import PartitionSpec as P

MESH = pl.DeviceIdType.MESH
NZ, NY, NX = 16, 4, 4
ROWS = 32
TOKENS = 256
D = 2048


def ring(name, count):
    me = lax.axis_index(name)

    def at(step):
        return lax.rem(me + (step % count), count)

    return at


def gather_project(
    tok, wv, wg, wq, wk, wl, gain, gate_w, gate_b,
    glu_o, q_o, k_o, v_o, gates_o,
    wa, wb, rows_in, normed, own,
    az_s, az_r, ay_s, ay_r, by_s, by_r, bz_s, bz_r, tx_s, tx_r, td_s, td_r,
):
    zat, yat, xat = ring("z", NZ), ring("y", NY), ring("x", NX)
    core = lax.axis_index("c")
    other = 1 - core

    def up_z(ref_s, ref_r, src, dst, way):
        return pltpu.make_async_remote_copy(src, dst, ref_s, ref_r, device_id={"z": zat(way)}, device_id_type=MESH)

    def up_y(ref_s, ref_r, src, dst, way):
        return pltpu.make_async_remote_copy(src, dst, ref_s, ref_r, device_id={"y": yat(way)}, device_id_type=MESH)

    def up_x(ref_s, ref_r, src, dst, way):
        return pltpu.make_async_remote_copy(src, dst, ref_s, ref_r, device_id={"x": xat(way)}, device_id_type=MESH)

    def across(ref_s, ref_r, src, dst):
        return pltpu.make_async_remote_copy(src, dst, ref_s, ref_r, device_id={"c": other}, device_id_type=MESH)

    def row_at(dz, dy):
        return pl.multiple_of((zat(dz) * NY + yat(dy)) * ROWS, ROWS)

    sent = []

    def go(copy):
        copy.start()
        sent.append(copy)
        return copy

    mine = row_at(0, 0)
    a_own = [wv, wg, wq]
    b_own = [wk, wl]
    loads = []
    for n, w in enumerate(a_own):
        loads.append(pltpu.make_async_copy(w, wa.at[pl.ds(mine, ROWS), pl.ds(256 * n, 256)], own.at[n]))
    for n, w in enumerate(b_own):
        loads.append(pltpu.make_async_copy(w, wb.at[pl.ds(mine, ROWS), pl.ds(256 * n, 256)], own.at[3 + n]))
    tp_own = xat(0) * 2 + core
    loads.append(pltpu.make_async_copy(tok, rows_in.at[tp_own], own.at[5]))
    for copy in loads:
        copy.start()

    barrier = pltpu.get_barrier_semaphore()
    for dev in ({"z": zat(1)}, {"z": zat(-1)}, {"y": yat(1)}, {"y": yat(-1)}, {"x": xat(1)}, {"x": xat(-1)}, {"c": other}):
        pl.semaphore_signal(barrier, inc=1, device_id=dev, device_id_type=MESH)
    pl.semaphore_wait(barrier, 7)

    def a_block(dz, dy, lo=0, size=ROWS):
        return wa.at[pl.ds(pl.multiple_of(row_at(dz, dy) + lo, 16), size), :]

    def b_block(dz, dy, lo=0, size=ROWS):
        return wb.at[pl.ds(pl.multiple_of(row_at(dz, dy) + lo, 16), size), :]

    def b_group(dz, lo=0, size=ROWS * NY):
        return wb.at[pl.ds(pl.multiple_of(zat(dz) * (ROWS * NY) + lo, 64), size), :]

    def send_az(way, s):
        sign = 1 if way == 0 else -1
        dz = -sign * (s - 1)
        if s < 8:
            block = a_block(dz, 0)
        else:
            block = a_block(dz, 0, 16 * way, 16)
        return go(up_z(az_s.at[way, s - 1], az_r.at[way, s - 1], block, block, sign))

    def send_bz(way, s):
        sign = 1 if way == 0 else -1
        dz = -sign * (s - 1)
        if s < 8:
            block = b_group(dz)
        else:
            block = b_group(dz, 64 * way, 64)
        return go(up_z(bz_s.at[way, s - 1], bz_r.at[way, s - 1], block, block, sign))

    def y_first(n, dz):
        block = a_block(dz, 0)
        return [go(up_y(ay_s.at[n, w], ay_r.at[n, w], block, block, 1 - 2 * w)) for w in range(2)]

    def y_second(n, dz, first):
        second = []
        for w in range(2):
            first[w].wait_recv()
            sign = 1 - 2 * w
            block = a_block(dz, -sign, 16 * w, 16)
            second.append(go(up_y(ay_s.at[n, 2 + w], ay_r.at[n, 2 + w], block, block, sign)))
        return second

    for copy in loads[:3]:
        copy.wait()
    az = [send_az(0, 1), send_az(1, 1)]
    for copy in loads[3:5]:
        copy.wait()
    by1 = []
    for w in range(2):
        block = b_block(0, 0)
        by1.append(go(up_y(by_s.at[w], by_r.at[w], block, block, 1 - 2 * w)))
    loads[5].wait()
    tx1 = []
    for w in range(2):
        block = rows_in.at[tp_own]
        tx1.append(go(up_x(tx_s.at[w], tx_r.at[w], block, block, 1 - 2 * w)))
    td = [go(across(td_s.at[0], td_r.at[0], rows_in.at[tp_own], rows_in.at[tp_own]))]
    ay_next = [(0, 0, y_first(0, 0))]

    by2 = []
    for w in range(2):
        by1[w].wait_recv()
        sign = 1 - 2 * w
        block = b_block(0, -sign, 16 * w, 16)
        by2.append(go(up_y(by_s.at[2 + w], by_r.at[2 + w], block, block, sign)))
    tx2 = []
    for w in range(2):
        tx1[w].wait_recv()
        sign = 1 - 2 * w
        slot = xat(-sign) * 2 + core
        half = rows_in.at[slot, pl.ds(128 * w, 128)]
        tx2.append(go(up_x(tx_s.at[2 + w], tx_r.at[2 + w], half, half, sign)))
        td.append(go(across(td_s.at[1 + w], td_r.at[1 + w], rows_in.at[slot], rows_in.at[slot])))
    for copy in by2:
        copy.wait_recv()
    bz = [send_bz(0, 1), send_bz(1, 1)]

    ay_last = []
    for s in range(1, 9):
        fresh = []
        for w in range(2):
            sign = 1 if w == 0 else -1
            az[w].wait_recv()
            if s < 8:
                az[w] = send_az(w, s + 1)
                n = s if w == 0 else 7 + s
                fresh.append((n, -sign * s, y_first(n, -sign * s)))
        if s == 8:
            fresh.append((15, 8, y_first(15, 8)))
        for w in range(2):
            bz[w].wait_recv()
            if s < 8:
                bz[w] = send_bz(w, s + 1)
        for n, dz, first in ay_next:
            ay_last.extend(y_second(n, dz, first))
        ay_next = fresh
        if s == 1:
            slot = xat(2) * 2 + core
            for w in range(2):
                tx2[w].wait_recv()
                half = rows_in.at[slot, pl.ds(128 * w, 128)]
                td.append(go(across(td_s.at[3 + w], td_r.at[3 + w], half, half)))
        if s == 2:
            for copy in td:
                copy.wait_recv()
            square = jnp.zeros((TOKENS, 256), jnp.float32)
            for b in range(8):
                wide = rows_in[b].astype(jnp.float32)
                square = square + wide * wide
            scale = lax.rsqrt(jnp.sum(square, axis=1, keepdims=True) / D + 1e-6)
            for b in range(8):
                cols = slice(256 * b, 256 * b + 256)
                normed[:, cols] = (rows_in[b].astype(jnp.float32) * scale * gain[:, cols]).astype(jnp.bfloat16)
            gates_o[...] = jnp.dot(normed[...], gate_w[...], preferred_element_type=jnp.float32) + gate_b[...]
    for n, dz, first in ay_next:
        ay_last.extend(y_second(n, dz, first))
    k_o[...] = jnp.dot(normed[...], wb[:, 0:256], preferred_element_type=jnp.float32).astype(jnp.bfloat16)
    v_o[...] = jnp.dot(normed[...], wb[:, 256:512], preferred_element_type=jnp.float32).astype(jnp.bfloat16)
    for copy in ay_last:
        copy.wait_recv()
    value = jnp.dot(normed[...], wa[:, 0:256], preferred_element_type=jnp.float32)
    gate = jnp.dot(normed[...], wa[:, 256:512], preferred_element_type=jnp.float32)
    glu_o[...] = (value * jax.nn.sigmoid(gate)).astype(jnp.bfloat16)
    q_o[...] = jnp.dot(normed[...], wa[:, 512:768], preferred_element_type=jnp.float32).astype(jnp.bfloat16)
    for copy in sent:
        copy.wait_send()


def projected(tokens, weights, norm_gain, gate_weight, gate_bias):
    vmem = pl.BlockSpec(memory_space=pltpu.VMEM)
    hbm = pl.BlockSpec(memory_space=pltpu.HBM)
    bf = jnp.bfloat16
    dma = pltpu.SemaphoreType.DMA
    return pl.pallas_call(
        gather_project,
        out_shape=[jax.ShapeDtypeStruct((TOKENS, 256), bf)] * 4 + [jax.ShapeDtypeStruct((TOKENS, 32), jnp.float32)],
        in_specs=[hbm] * 6 + [vmem] * 3,
        out_specs=[vmem] * 5,
        scratch_shapes=[
            pltpu.VMEM((D, 768), bf),
            pltpu.VMEM((D, 512), bf),
            pltpu.VMEM((8, TOKENS, 256), bf),
            pltpu.VMEM((TOKENS, D), bf),
            dma((6,)),
            dma((2, 8)), dma((2, 8)),
            dma((16, 4)), dma((16, 4)),
            dma((4,)), dma((4,)),
            dma((2, 8)), dma((2, 8)),
            dma((4,)), dma((4,)),
            dma((5,)), dma((5,)),
        ],
        compiler_params=pltpu.CompilerParams(collective_id=0, has_side_effects=True, vmem_limit_bytes=40 * 1024 * 1024),
        name="gather_project",
    )(tokens, *weights, norm_gain.reshape(1, D), gate_weight, gate_bias.reshape(1, 32))
NEG = -1e30
EPS = 1e-06
F32 = jnp.float32
BF16 = jnp.bfloat16


def joined(state, level, new_state, new_level, decay):
    top = jnp.maximum(level + decay, new_level)
    early = jnp.exp(level + decay - top)
    late = jnp.exp(new_level - top)
    parts = []
    for old, new in zip(state, new_state):
        if old.ndim == 3:
            parts.append(early[None] * old + late[None] * new)
        else:
            parts.append(early * old + late * new)
    return tuple(parts), top


def log_sigmoid(x):
    return -(jnp.maximum(-x, 0.0) + jnp.log1p(jnp.exp(-jnp.abs(x))))


def mix(
    glu, q, k, v, gates, extra, taps, ln_gain, ln_bias, mem_gain, out_conv, out_mem,
    out,
    wc, wm, st, sm, ry, rsm, tz, gsm, rz, rgs, iz, ri, inc, rin,
    halo, ext, cv, stat, rstat, act, mem, num_f, num_b, psend, pown, precv, xsend, xrecv,
    wsem, h_s, h_r, y_s, y_r, ym_s, ym_r, z_s, z_r, zm_s, zm_r, zb_s, zb_r, yb_s, yb_r, t_s, t_r, d_s, d_r, o_s, o_r,
):
    zat, yat, xat = ring("z", NZ), ring("y", NY), ring("x", NX)
    z, y, x, core = lax.axis_index("z"), lax.axis_index("y"), lax.axis_index("x"), lax.axis_index("c")
    other = 1 - core
    head = x * 2 + core

    def remote(src, dst, ss, rs, dev):
        return pltpu.make_async_remote_copy(src, dst, ss, rs, device_id=dev, device_id_type=MESH)

    sent = []

    def go(copy):
        copy.start()
        sent.append(copy)
        return copy

    wide = [pltpu.make_async_copy(out_conv, wc, wsem.at[0]), pltpu.make_async_copy(out_mem, wm, wsem.at[1])]
    for copy in wide:
        copy.start()

    after = {"z": zat(lax.convert_element_type(y == NY - 1, jnp.int32)), "y": yat(1)}
    before = {"z": lax.rem(z + NZ - lax.convert_element_type(y == 0, jnp.int32), NZ), "y": yat(-1)}
    peers = [after, before]
    peers += [{"y": yat(dy)} for dy in range(1, NY)]
    peers += [{"z": zat(dz)} for dz in range(1, NZ)]
    peers += [{"x": xat(dx), "c": cc} for dx in range(1, NX) for cc in (core, other)] + [{"c": other}]
    barrier = pltpu.get_barrier_semaphore()
    for dev in peers:
        pl.semaphore_signal(barrier, inc=1, device_id=dev, device_id_type=MESH)

    lane = lax.broadcasted_iota(jnp.int32, (TOKENS, 32), 1)
    lane16 = lax.broadcasted_iota(jnp.int32, (TOKENS, 16), 1)
    t_at = lax.broadcasted_iota(jnp.int32, (TOKENS, TOKENS), 0)
    s_at = lax.broadcasted_iota(jnp.int32, (TOKENS, TOKENS), 1)

    def column(n):
        return jnp.sum(jnp.where(lane == 8 * n + head, gates[...], 0.0), axis=1, keepdims=True)

    def extra_column(n):
        return jnp.sum(jnp.where(lane16 == 8 * n + head, extra[...], 0.0), axis=1, keepdims=True)

    def as_row(col):
        return jnp.sum(jnp.where(t_at == s_at, col, 0.0), axis=0, keepdims=True)

    def as_column(row):
        return jnp.sum(jnp.where(t_at == s_at, row, 0.0), axis=1, keepdims=True)

    in_f, in_b = column(0), column(2)
    lf_f = log_sigmoid(column(1)) + extra_column(0)
    lf_b = log_sigmoid(column(3)) + extra_column(1)
    sum_f_row = jnp.sum(jnp.where(t_at <= s_at, lf_f, 0.0), axis=0, keepdims=True)
    sum_b_row = jnp.sum(jnp.where(t_at >= s_at, lf_b, 0.0), axis=0, keepdims=True)
    sum_f, sum_b = as_column(sum_f_row), as_column(sum_b_row)
    total_f = jnp.sum(lf_f, axis=0, keepdims=True)
    total_b = jnp.sum(lf_b, axis=0, keepdims=True)

    keys = k[...].astype(F32)

    def summary(total, sums, gate):
        to_end = total - sums + gate
        level = jnp.max(to_end, axis=0, keepdims=True)
        weighted = keys * (jnp.exp(to_end - level) * 0.0625)
        state = lax.dot_general(weighted.astype(BF16), v[...], (((0,), (0,)), ((), ())), preferred_element_type=F32)
        return state, jnp.sum(weighted, axis=0, keepdims=True), level

    state_f, vec_f, level_f = summary(total_f, sum_f, in_f)
    state_b, vec_b, level_b = summary(total_b, sum_b, in_b)
    for h in range(2):
        cols = slice(128 * h, 128 * h + 128)
        both = jnp.concatenate([state_f[:, cols].reshape(32, 8, 128), state_b[:, cols].reshape(32, 8, 128)], axis=1)
        st[32 * h : 32 * h + 32] = both.astype(BF16)
    for n, row in enumerate((vec_f[:, :128], vec_f[:, 128:], vec_b[:, :128], vec_b[:, 128:])):
        sm[n : n + 1, :] = row
    for n, one in enumerate((total_f, level_f, total_b, level_b)):
        sm[4 + n : 5 + n, :] = jnp.broadcast_to(one, (1, 128))
    ry[y] = st[pl.ds(y * 16, 16)]
    rsm[y] = sm[...]

    pl.semaphore_wait(barrier, len(peers))
    halos = [
        go(remote(glu.at[pl.ds(240, 16), :], halo.at[0], h_s.at[0], h_r.at[0], after)),
        go(remote(glu.at[pl.ds(0, 16), :], halo.at[1], h_s.at[1], h_r.at[1], before)),
    ]
    y_in = []
    for dy in range(1, NY):
        to = yat(dy)
        y_in.append(go(remote(sm, rsm.at[y], ym_s.at[dy], ym_r.at[dy], {"y": to})))
        y_in.append(go(remote(st.at[pl.ds(to * 16, 16)], ry.at[y], y_s.at[dy], y_r.at[dy], {"y": to})))

    scores = lax.dot_general(q[...], k[...], (((1,), (1,)), ((), ())), preferred_element_type=F32) * 0.0625

    def inside(mask, sums, sum_row, gate, numerator):
        log_weight = jnp.where(mask, sums - sum_row + as_row(gate), NEG)
        top = jnp.max(log_weight, axis=1, keepdims=True)
        weights = scores * jnp.exp(log_weight - top)
        numerator[...] = jnp.dot(weights.astype(BF16), v[...], preferred_element_type=F32)
        return jnp.sum(weights, axis=1, keepdims=True), top

    den_f, top_f = inside(s_at <= t_at, sum_f, sum_f_row, in_f, num_f)
    den_b, top_b = inside(s_at >= t_at, sum_b, sum_b_row, in_b, num_b)

    for copy in y_in:
        copy.wait_recv()

    def y_pieces(n, d):
        return ry[n].astype(F32)[:, 8 * d : 8 * d + 8, :], rsm[n, 2 * d : 2 * d + 2, :]

    def y_scalars(n, d):
        return rsm[n, 5 + 2 * d : 6 + 2 * d, :], rsm[n, 4 + 2 * d : 5 + 2 * d, :]

    def y_walk(d, start, level):
        state = start
        found = []
        for n in range(NY) if d == 0 else reversed(range(NY)):
            found.append((n, state, level))
            state, level = joined(state, level, y_pieces(n, d), *y_scalars(n, d))
        return found, state, level

    low = jnp.full((1, 128), NEG, F32)
    zero = (jnp.zeros((16, 8, 128), F32), jnp.zeros((2, 128), F32))
    groups = []
    for d in range(2):
        _, group, level = y_walk(d, zero, low)
        groups.append(group)
        gsm[2 * d : 2 * d + 2, :] = group[1]
        decay = low * 0.0
        for n in range(NY):
            decay = decay + y_scalars(n, d)[1]
        gsm[4 + 2 * d : 5 + 2 * d, :] = decay
        gsm[5 + 2 * d : 6 + 2 * d, :] = level
    tz[...] = jnp.concatenate([groups[0][0], groups[1][0]], axis=1).astype(BF16)
    rz[z] = tz[z]
    rgs[z] = gsm[...]
    z_in = []
    for dz in range(1, NZ):
        to = zat(dz)
        z_in.append(go(remote(tz.at[to], rz.at[z], z_s.at[dz], z_r.at[dz], {"z": to})))
        z_in.append(go(remote(gsm, rgs.at[z], zm_s.at[dz], zm_r.at[dz], {"z": to})))

    for copy in halos:
        copy.wait_recv()
    place = z * NY + y
    for h in range(2):
        cols = slice(128 * h, 128 * h + 128)
        ext[h, 0:16, :] = jnp.where(place == 0, 0.0, halo[0][:, cols].astype(F32))
        ext[h, 16:272, :] = glu[:, cols].astype(F32)
        ext[h, 272:288, :] = jnp.where(place == NZ * NY - 1, 0.0, halo[1][:, cols].astype(F32))
    for h in range(2):
        cols = slice(128 * h, 128 * h + 128)

        def rows_of(n, carry):
            first = n * 64
            total = jnp.zeros((64, 128), F32)
            for j in range(31):
                total = total + taps[j : j + 1, cols] * ext[h, pl.ds(first + (j + 1), 64), :]
            cv[pl.ds(pl.multiple_of(first, 64), 64), cols] = total
            return carry

        lax.fori_loop(0, 4, rows_of, 0)
    conv = cv[...]
    stat[0:1, :] = as_row(jnp.sum(conv, axis=1, keepdims=True))
    stat[1:2, :] = as_row(jnp.sum(conv * conv, axis=1, keepdims=True))
    stat[2:8, :] = jnp.zeros((6, TOKENS), F32)
    t_in = []
    tp_peers = [(dx, cc) for dx in range(NX) for cc in range(2) if dx or cc]
    for n, (dx, cc) in enumerate(tp_peers):
        dev = {"x": xat(dx), "c": core if cc == 0 else other}
        t_in.append(go(remote(stat, rstat.at[n], t_s.at[n], t_r.at[n], dev)))

    for copy in z_in:
        copy.wait_recv()
    came, came_level = [], []
    entering = []
    for d in range(2):
        state = (jnp.zeros((8, 128), F32), jnp.zeros((2, 128), F32))
        level = low
        kept, kept_level = jnp.zeros((2, 128), F32), low
        lines = [None] * NZ
        for n in range(NZ) if d == 0 else reversed(range(NZ)):
            lines[n] = state[0]
            kept = jnp.where(z == n, state[1], kept)
            kept_level = jnp.where(z == n, level, kept_level)
            piece = (rz[n].astype(F32)[8 * d : 8 * d + 8, :], rgs[n, 2 * d : 2 * d + 2, :])
            state, level = joined(state, level, piece, rgs[n, 5 + 2 * d : 6 + 2 * d, :], rgs[n, 4 + 2 * d : 5 + 2 * d, :])
        entering.append(lines)
        came.append(kept)
        came_level.append(kept_level)
    for n in range(NZ):
        iz[n] = jnp.concatenate([entering[0][n], entering[1][n]], axis=0).astype(BF16)
    ri[z] = iz[z]
    zb_in = []
    for dz in range(1, NZ):
        to = zat(dz)
        zb_in.append(go(remote(iz.at[to], ri.at[z], zb_s.at[dz], zb_r.at[dz], {"z": to})))

    sums = stat[...]
    for n, copy in enumerate(t_in):
        copy.wait_recv()
        sums = sums + rstat[n]
    mean = as_column(sums[0:1, :]) / CONV
    var = as_column(sums[1:2, :]) / CONV - mean * mean
    normal = (cv[...] - mean) * lax.rsqrt(var + EPS) * ln_gain[...] + ln_bias[...]
    act[...] = (normal * jax.nn.sigmoid(normal)).astype(BF16).reshape(8, 32, 256)
    for copy in wide:
        copy.wait()

    for copy in zb_in:
        copy.wait_recv()
    back = [None] * 2
    mine = []
    for d in range(2):
        start = (ri[...].astype(F32)[:, 8 * d : 8 * d + 8, :], came[d])
        found, _, _ = y_walk(d, start, came_level[d])
        kept, kept_level = jnp.zeros((2, 128), F32), low
        back[d] = [None] * NY
        for n, state, level in found:
            back[d][n] = state[0]
            kept = jnp.where(y == n, state[1], kept)
            kept_level = jnp.where(y == n, level, kept_level)
        mine.append((kept, kept_level))
    for n in range(NY):
        inc[n] = jnp.concatenate([back[0][n], back[1][n]], axis=1).astype(BF16)
    rin[y] = inc[y]
    yb_in = []
    for dy in range(1, NY):
        to = yat(dy)
        yb_in.append(go(remote(inc.at[to], rin.at[y], yb_s.at[dy], yb_r.at[dy], {"y": to})))
    for copy in yb_in:
        copy.wait_recv()

    def finished(d, numerator, den, top, sums):
        vec, level = mine[d]
        vec = jnp.concatenate([vec[0:1, :], vec[1:2, :]], axis=1)
        state = rin[...].reshape(64, 16, 128).astype(F32)[:, 8 * d : 8 * d + 8, :]
        left = state[:32].reshape(256, 128).astype(BF16)
        right = state[32:].reshape(256, 128).astype(BF16)
        carried = sums + level[:, 0:1]
        high = jnp.maximum(top, carried)
        near = jnp.exp(top - high)
        far = jnp.exp(carried - high)
        read = jnp.concatenate(
            [jnp.dot(q[...], left, preferred_element_type=F32), jnp.dot(q[...], right, preferred_element_type=F32)], axis=1
        )
        upper = near * numerator[...] + far * read
        lower = near * den + far * jnp.sum(q[...].astype(F32) * vec, axis=1, keepdims=True)
        return upper / jnp.maximum(jnp.abs(lower), jnp.exp(-high))

    summed = finished(0, num_f, den_f, top_f, sum_f) + finished(1, num_b, den_b, top_b, sum_b)
    scale = lax.rsqrt(jnp.mean(summed * summed, axis=1, keepdims=True) + EPS)
    mem[...] = (summed * scale * mem_gain[...]).astype(BF16).reshape(8, 32, 256)

    def part(c, dx):
        slot = xat(dx) * 2 + c
        return jnp.dot(act[slot], wc[...], preferred_element_type=F32) + jnp.dot(mem[slot], wm[...], preferred_element_type=F32)

    d_in = []
    order = (2, 1, 3, 0)
    for dx in order:
        psend[dx] = part(other, dx).astype(BF16)
        d_in.append(go(remote(psend.at[dx], precv.at[dx], d_s.at[dx], d_r.at[dx], {"c": other})))
    o_in = []
    for n, dx in enumerate(order):
        own = part(core, dx)
        d_in[n].wait_recv()
        own = own + precv[dx].astype(F32)
        if dx:
            xsend[dx] = own.astype(BF16)
            o_in.append(go(remote(xsend.at[dx], xrecv.at[dx], o_s.at[dx], o_r.at[dx], {"x": xat(dx)})))
        else:
            pown[...] = own
    total = pown[...]
    for copy, dx in zip(o_in, order):
        copy.wait_recv()
        total = total + xrecv[dx].astype(F32)
    out[...] = total.astype(BF16)
    for copy in sent:
        copy.wait_send()


def mixed_rows(glu, q, k, v, gates, extra, taps, ln_gain, ln_bias, mem_gain, out_conv, out_mem):
    vmem = pl.BlockSpec(memory_space=pltpu.VMEM)
    hbm = pl.BlockSpec(memory_space=pltpu.HBM)
    dma = pltpu.SemaphoreType.DMA
    V = pltpu.VMEM
    return pl.pallas_call(
        mix,
        out_shape=jax.ShapeDtypeStruct((32, D), BF16),
        in_specs=[vmem] * 10 + [hbm] * 2,
        out_specs=vmem,
        scratch_shapes=[
            V((256, D), BF16), V((256, D), BF16),
            V((64, 16, 128), BF16), V((8, 128), F32),
            V((4, 16, 16, 128), BF16), V((4, 8, 128), F32),
            V((16, 16, 128), BF16), V((8, 128), F32),
            V((16, 16, 128), BF16), V((16, 8, 128), F32),
            V((16, 16, 128), BF16), V((16, 16, 128), BF16),
            V((4, 16, 16, 128), BF16), V((4, 16, 16, 128), BF16),
            V((2, 16, 256), BF16), V((2, 288, 128), F32), V((256, 256), F32),
            V((8, 256), F32), V((7, 8, 256), F32),
            V((8, 32, 256), BF16), V((8, 32, 256), BF16),
            V((256, 256), F32), V((256, 256), F32),
            V((4, 32, D), BF16), V((32, D), F32), V((4, 32, D), BF16), V((4, 32, D), BF16), V((4, 32, D), BF16),
            dma((2,)),
            dma((2,)), dma((2,)),
            dma((4,)), dma((4,)), dma((4,)), dma((4,)),
            dma((16,)), dma((16,)), dma((16,)), dma((16,)), dma((16,)), dma((16,)),
            dma((4,)), dma((4,)),
            dma((7,)), dma((7,)),
            dma((4,)), dma((4,)), dma((4,)), dma((4,)),
        ],
        compiler_params=pltpu.CompilerParams(collective_id=1, has_side_effects=True, vmem_limit_bytes=48 * 1024 * 1024),
        name="mix",
    )(glu, q, k, v, gates, extra, taps, ln_gain.reshape(1, 256), ln_bias.reshape(1, 256), mem_gain.reshape(1, 256), out_conv, out_mem)


CONV = 2048


def shards(
    tokens,
    norm_gain,
    glu_value,
    glu_gate,
    conv_taps,
    ln_gain,
    ln_bias,
    query_weight,
    key_weight,
    value_weight,
    gate_weight,
    gate_bias,
    log_decay_extra,
    mem_gain,
    out_conv,
    out_mem,
):
    glu, q, k, v, gates = projected(
        tokens, (glu_value, glu_gate, query_weight, key_weight, value_weight), norm_gain, gate_weight, gate_bias
    )
    return mixed_rows(glu, q, k, v, gates, log_decay_extra, conv_taps, ln_gain, ln_bias, mem_gain, out_conv, out_mem)


SP = ("z", "y")
TP = ("x", "c")


def solution(mesh):
    split = Mesh(mesh.devices.reshape(NZ, NY, NX, 2), ("z", "y", "x", "c"))
    placed = (
        P(SP, TP),
        P(),
        P(SP, TP),
        P(SP, TP),
        P(None, TP),
        P(TP),
        P(TP),
        P(SP, TP),
        P(SP, TP),
        P(SP, TP),
        P(),
        P(),
        P(SP, None),
        P(TP),
        P(TP, None),
        P(TP, None),
    )
    return jax.shard_map(shards, mesh=split, in_specs=placed, out_specs=P(SP + TP, None), check_vma=False)
```

```python
import jax
import jax.numpy as jnp
from jax import lax
from jax.experimental import pallas as pl
from jax.experimental.pallas import tpu as pltpu
from jax.sharding import Mesh
from jax.sharding import PartitionSpec as P

MESH = pl.DeviceIdType.MESH
NZ, NY, NX = 16, 4, 4
ROWS = 32
TOKENS = 256
D = 2048
CONV = 2048
NEG = -1e30
EPS = 1e-06
F32 = jnp.float32
BF16 = jnp.bfloat16


def joined(state, level, new_state, new_level, decay):
    top = jnp.maximum(level + decay, new_level)
    early = jnp.exp(level + decay - top)
    late = jnp.exp(new_level - top)
    parts = []
    for old, new in zip(state, new_state):
        if old.ndim == 3:
            parts.append(early[None] * old + late[None] * new)
        else:
            parts.append(early * old + late * new)
    return tuple(parts), top


def log_sigmoid(x):
    return -(jnp.maximum(-x, 0.0) + jnp.log1p(jnp.exp(-jnp.abs(x))))


def ring(name, count):
    me = lax.axis_index(name)

    def at(step):
        return lax.rem(me + (step % count), count)

    return at


def remote(src, dst, ss, rs, dev):
    return pltpu.make_async_remote_copy(src, dst, ss, rs, device_id=dev, device_id_type=MESH)


GROUPS = ((2, ((6, 5),)), (4, ((11, 2), (4, 2))), (6, ((13, 2), (2, 2))), (8, ((15, 1), (0, 2))))


class ZThenY:
    def __init__(self, plan, go, w, z_sem, y_sem, z_out, y_out, base, hop, side):
        self.plan, self.go, self.w = plan, go, w
        self.z_sem, self.y_sem, self.z_out, self.y_out = z_sem, y_sem, z_out, y_out
        self.zat, self.yat = ring("z", NZ), ring("y", NY)
        self.y = lax.axis_index("y")
        self.base, self.hop, self.side = base, hop, side
        self.late = []
        self.count = 0

    def begin(self):
        for way in range(2):
            self.along(way, 1)

    def along(self, way, s):
        sign = 1 - 2 * way
        src, dst = 8 + sign * (s - 1), (8 + sign * s) % 16
        if s < 8:
            src, dst = self.w.at[src, self.y], self.w.at[dst, self.y]
        else:
            src, dst = self.w.at[src, self.y, pl.ds(16 * way, 16)], self.w.at[dst, self.y, pl.ds(16 * way, 16)]
        copy = self.go(src, dst, self.z_out, self.z_sem.at[way, s - 1], {"z": self.zat(sign)})
        now = self.base + self.hop * s

        def landed():
            copy.wait_recv()
            if s < 8:
                self.along(way, s + 1)
            if way == 1:
                for last, ranges in GROUPS:
                    if last == s:
                        for first, count in ranges:
                            self.spread(first, count, now)

        self.plan(now, landed)

    def spread(self, first, count, now):
        n = self.count
        self.count += 1
        block = self.w.at[pl.ds(first, count), self.y]
        for way in range(2):
            sign = 1 - 2 * way
            copy = self.go(block, block, self.y_out, self.y_sem.at[n, way], {"y": self.yat(sign)})

            def landed(way=way, sign=sign, copy=copy):
                copy.wait_recv()
                half = self.w.at[pl.ds(first, count), self.yat(-sign), pl.ds(16 * way, 16)]
                self.late.append(self.go(half, half, self.y_out, self.y_sem.at[n, 2 + way], {"y": self.yat(sign)}))

            self.plan(now + self.side + 0.7 * count, landed)

    def end(self):
        for copy in self.late:
            copy.wait_recv()


class YThenZ:
    def __init__(self, plan, go, w, y_sem, z_sem, out, base, hop, side):
        self.plan, self.go, self.w, self.y_sem, self.z_sem, self.out = plan, go, w, y_sem, z_sem, out
        self.zat, self.yat = ring("z", NZ), ring("y", NY)
        self.base, self.hop, self.side = base, hop, side
        self.far, self.late = [], []

    def begin(self, now):
        block = self.w.at[32 + lax.axis_index("y")]
        for way in range(2):
            sign = 1 - 2 * way
            copy = self.go(block, block, self.out, self.y_sem.at[way], {"y": self.yat(sign)})

            def landed(way=way, sign=sign, copy=copy):
                copy.wait_recv()
                half = self.w.at[32 + self.yat(-sign), pl.ds(16 * way, 16)]
                self.far.append(self.go(half, half, self.out, self.y_sem.at[2 + way], {"y": self.yat(sign)}))

            self.plan(now + self.side, landed)

    def begin_z(self):
        for copy in self.far:
            copy.wait_recv()
        for way in range(2):
            self.along(way, 1)

    def along(self, way, s):
        sign = 1 - 2 * way
        src, dst = 8 + sign * (s - 1), (8 + sign * s) % 16
        if s < 8:
            src, dst = self.w.at[pl.ds(4 * src, 4)], self.w.at[pl.ds(4 * dst, 4)]
        else:
            src, dst = self.w.at[pl.ds(4 * src + 2 * way, 2)], self.w.at[pl.ds(4 * dst + 2 * way, 2)]
        copy = self.go(src, dst, self.out, self.z_sem.at[way, s - 1], {"z": self.zat(sign)})
        if s == 8:
            self.late.append(copy)
            return

        def landed():
            copy.wait_recv()
            self.along(way, s + 1)

        self.plan(self.base + self.hop * s, landed)

    def end(self):
        for copy in self.late:
            copy.wait_recv()


def layer(
    tok, wv, wg, wq, wk, wl, gain_h, gate_h, bias_h, extra_h, taps_h, lng_h, lnb_h, memg_h, oc_h, om_h,
    out,
    w_kv, w_glu, w_q, rows_in, normed,
    gain, gate_w, gate_r, gate_b, extra, taps, ln_gain, ln_bias, mem_gain, wc, wm,
    glu, q, k, v,
    st, sm, ry, rsm, tz, gsm, rz, rgs, iz, ri, inc, rin,
    halo, ext, cv, stat, rstat, act, mem, num_f, num_b,
    psend, precv, xfar, xnear, xsum, rfar, rnear, rsum, pair,
    own, out_sem, kv_z, kv_y, glu_z, glu_y, q_y, q_z, tx_r, td_r, h_r, step_r, d_r, o_r,
):
    zat, yat, xat = ring("z", NZ), ring("y", NY), ring("x", NX)
    z, y, x, core = lax.axis_index("z"), lax.axis_index("y"), lax.axis_index("x"), lax.axis_index("c")
    other = 1 - core
    head = x * 2 + core
    sent = [0] * 12

    def go(src, dst, out_to, landed, dev):
        copy = remote(src, dst, out_sem.at[out_to], landed, dev)
        copy.start()
        size = 1
        for n in src.shape:
            size *= n
        sent[out_to] += size * jnp.dtype(src.dtype).itemsize
        return copy

    def all_of(ref, sem):
        pltpu.make_async_copy(ref, ref, sem).wait()

    def load(src, dst, n):
        copy = pltpu.make_async_copy(src, dst, own.at[n])
        copy.start()
        return copy

    l_kv = [load(src, w_kv.at[8, y, :, pl.ds(256 * n, 256)], n) for n, src in enumerate((wk, wl))]
    l_tok = load(tok, rows_in.at[head], 2)
    l_rest = [load(src, w_glu.at[8, y, :, pl.ds(256 * n, 256)], 3 + n) for n, src in enumerate((wv, wg))]
    l_q = load(wq, w_q.at[32 + y], 5)
    small = [(gain_h, gain), (gate_h, gate_w), (bias_h, gate_b), (extra_h, extra), (taps_h, taps), (lng_h, ln_gain),
             (lnb_h, ln_bias), (memg_h, mem_gain), (oc_h, wc), (om_h, wm)]
    small = [load(src, dst, 6 + n) for n, (src, dst) in enumerate(small)]

    barrier = pltpu.get_barrier_semaphore()
    greeted = [{"z": zat(1)}, {"z": zat(-1)}, {"y": yat(1)}, {"y": yat(-1)}, {"x": xat(1)}, {"x": xat(-1)}, {"c": other}]
    for dev in greeted:
        pl.semaphore_signal(barrier, inc=1, device_id=dev, device_id_type=MESH)
    pl.semaphore_wait(barrier, len(greeted))

    tasks = []
    later = {}

    def plan(when, act_on):
        tasks.append((when, len(tasks), act_on))

    def run():
        while tasks:
            item = min(tasks, key=lambda t: t[:2])
            tasks.remove(item)
            item[2]()

    for copy in l_kv:
        copy.wait()
    kv = ZThenY(plan, go, w_kv, kv_z, kv_y, 0, 1, 0.0, HOP1, SIDE1)
    kv.begin()
    values = ZThenY(plan, go, w_glu, glu_z, glu_y, 2, 3, T2, HOP2, SIDE2)
    query = YThenZ(plan, go, w_q, q_y, q_z, 4, T2, HOP2, SIDE2)

    def tokens_out():
        l_tok.wait()
        block = rows_in.at[head]
        later["tx"] = [go(block, block, 5, tx_r.at[w], {"x": xat(1 - 2 * w)}) for w in range(2)]
        later["td"] = [go(block, block, 5, td_r.at[0], {"c": other})]
        l_q.wait()
        query.begin(0.1)

    def tokens_on():
        later["tx2"] = []
        for w in range(2):
            later["tx"][w].wait_recv()
            sign = 1 - 2 * w
            slot = xat(-sign) * 2 + core
            half = rows_in.at[slot, pl.ds(128 * w, 128)]
            later["tx2"].append(go(half, half, 5, tx_r.at[2 + w], {"x": xat(sign)}))
            later["td"].append(go(rows_in.at[slot], rows_in.at[slot], 5, td_r.at[1 + w], {"c": other}))

    def tokens_far():
        slot = xat(2) * 2 + core
        for w in range(2):
            later["tx2"][w].wait_recv()
            half = rows_in.at[slot, pl.ds(128 * w, 128)]
            later["td"].append(go(half, half, 5, td_r.at[3 + w], {"c": other}))

    def tokens_in():
        for copy in later["td"]:
            copy.wait_recv()
        for copy in small:
            copy.wait()
        square = jnp.zeros((TOKENS, 256), F32)
        for b in range(8):
            wide = rows_in[b].astype(F32)
            square = square + wide * wide
        scale = lax.rsqrt(jnp.sum(square, axis=1, keepdims=True) / D + EPS)
        for p in range(16):
            at_z = zat(8 - p)
            cols = pl.ds(pl.multiple_of(at_z * 128, 128), 128)
            part = rows_in[at_z // 2, :, pl.ds(pl.multiple_of((at_z % 2) * 128, 128), 128)].astype(F32)
            normed[:, 128 * p : 128 * p + 128] = (part * scale * gain[:, cols]).astype(BF16)
            gate_r[:, 128 * p : 128 * p + 128] = gate_w[:, cols]

    plan(0.0, tokens_out)
    plan(3.5, tokens_on)
    plan(7.0, tokens_far)
    plan(10.1, tokens_in)

    sub = lax.broadcasted_iota(jnp.int32, (32, TOKENS), 0)
    sub16 = lax.broadcasted_iota(jnp.int32, (16, TOKENS), 0)
    t_at = lax.broadcasted_iota(jnp.int32, (TOKENS, TOKENS), 0)
    s_at = lax.broadcasted_iota(jnp.int32, (TOKENS, TOKENS), 1)

    def as_row(col):
        return jnp.sum(jnp.where(t_at == s_at, col, 0.0), axis=0, keepdims=True)

    def as_column(row):
        return jnp.sum(jnp.where(t_at == s_at, row, 0.0), axis=1, keepdims=True)

    def ends(total, sum_row, gate):
        to_end = total - sum_row + gate
        level = jnp.max(to_end, axis=1, keepdims=True)
        return as_column(jnp.exp(to_end - level) * 0.0625), level

    def gates_in():
        diagonal = lax.broadcasted_iota(jnp.int32, (32, 32), 0) == lax.broadcasted_iota(jnp.int32, (32, 32), 1)
        bias = jnp.sum(jnp.where(diagonal, gate_b[...], 0.0), axis=1, keepdims=True)
        gates = lax.dot_general(gate_r[...], normed[...], (((1,), (1,)), ((), ())), preferred_element_type=F32) + bias

        def gate_row(n):
            return jnp.sum(jnp.where(sub == 8 * n + head, gates, 0.0), axis=0, keepdims=True)

        def extra_row(n):
            return jnp.sum(jnp.where(sub16 == 8 * n + head, extra[...], 0.0), axis=0, keepdims=True)

        later["rows"] = gate_row(0), gate_row(2)
        lf_f = log_sigmoid(gate_row(1)) + extra_row(0)
        lf_b = log_sigmoid(gate_row(3)) + extra_row(1)
        sum_f = jnp.sum(jnp.where(s_at <= t_at, lf_f, 0.0), axis=1, keepdims=True)
        sum_b = jnp.sum(jnp.where(s_at >= t_at, lf_b, 0.0), axis=1, keepdims=True)
        sum_f_row, sum_b_row = as_row(sum_f), as_row(sum_b)
        later["sums"] = sum_f, sum_f_row, sum_b, sum_b_row
        total_f = jnp.sum(lf_f, axis=1, keepdims=True)
        total_b = jnp.sum(lf_b, axis=1, keepdims=True)
        end_f, level_f = ends(total_f, sum_f_row, later["rows"][0])
        end_b, level_b = ends(total_b, sum_b_row, later["rows"][1])
        later["ends"] = end_f, end_b
        for n, one in enumerate((total_f, level_f, total_b, level_b)):
            sm[4 + n : 5 + n, :] = jnp.broadcast_to(one, (1, 128))

    plan(12.1, gates_in)

    def rest_out():
        for copy in l_rest:
            copy.wait()
        values.begin()
        query.begin_z()

    plan(T2, rest_out)

    def project(w, n):
        return jnp.dot(normed[...], w[:, :, :, 256 * n : 256 * n + 256].reshape(D, 256), preferred_element_type=F32)

    def states_out():
        kv.end()
        v[...] = project(w_kv, 1).astype(BF16)
        keys = project(w_kv, 0).astype(BF16)
        k[...] = keys
        keys = keys.astype(F32)

        def summary(end):
            weighted = keys * end
            state = lax.dot_general(weighted.astype(BF16), v[...], (((0,), (0,)), ((), ())), preferred_element_type=F32)
            return state, jnp.sum(weighted, axis=0, keepdims=True)

        state_f, vec_f = summary(later["ends"][0])
        state_b, vec_b = summary(later["ends"][1])
        for h in range(2):
            cols = slice(128 * h, 128 * h + 128)
            both = jnp.concatenate([state_f[:, cols].reshape(32, 8, 128), state_b[:, cols].reshape(32, 8, 128)], axis=1)
            st[32 * h : 32 * h + 32] = both.astype(BF16)
        for n, row in enumerate((vec_f[:, :128], vec_f[:, 128:], vec_b[:, :128], vec_b[:, 128:])):
            sm[n : n + 1, :] = row
        ry[y] = st[pl.ds(y * 16, 16)]
        rsm[y] = sm[...]
        for dy in (2, 1, 3):
            to = yat(dy)
            go(sm, rsm.at[y], 6, step_r.at[0], {"y": to})
            go(st.at[pl.ds(to * 16, 16)], ry.at[y], 6, step_r.at[1], {"y": to})

    plan(TS, states_out)

    def y_pieces(n, d):
        return ry[n].astype(F32)[:, 8 * d : 8 * d + 8, :], rsm[n, 2 * d : 2 * d + 2, :]

    def y_scalars(n, d):
        return rsm[n, 5 + 2 * d : 6 + 2 * d, :], rsm[n, 4 + 2 * d : 5 + 2 * d, :]

    def y_walk(d, start, level):
        state = start
        found = []
        for n in range(NY) if d == 0 else reversed(range(NY)):
            found.append((n, state, level))
            state, level = joined(state, level, y_pieces(n, d), *y_scalars(n, d))
        return found, state, level

    low = jnp.full((1, 128), NEG, F32)
    far_first = (8, 7, 9, 6, 10, 5, 11, 4, 12, 3, 13, 2, 14, 1, 15)

    def groups_out():
        all_of(rsm.at[pl.ds(0, 3)], step_r.at[0])
        all_of(ry.at[pl.ds(0, 3)], step_r.at[1])
        zero = (jnp.zeros((16, 8, 128), F32), jnp.zeros((2, 128), F32))
        groups = []
        for d in range(2):
            _, group, level = y_walk(d, zero, low)
            groups.append(group)
            gsm[2 * d : 2 * d + 2, :] = group[1]
            decay = low * 0.0
            for n in range(NY):
                decay = decay + y_scalars(n, d)[1]
            gsm[4 + 2 * d : 5 + 2 * d, :] = decay
            gsm[5 + 2 * d : 6 + 2 * d, :] = level
        tz[...] = jnp.concatenate([groups[0][0], groups[1][0]], axis=1).astype(BF16)
        rz[z] = tz[z]
        rgs[z] = gsm[...]
        for dz in far_first:
            to = zat(dz)
            go(tz.at[to], rz.at[z], 10, step_r.at[2], {"z": to})
            go(gsm, rgs.at[z], 10, step_r.at[3], {"z": to})

    plan(TY, groups_out)

    def pieces_back():
        all_of(rz.at[pl.ds(0, 15)], step_r.at[2])
        all_of(rgs.at[pl.ds(0, 15)], step_r.at[3])
        later["came"], later["came_level"] = [], []
        entering = []
        for d in range(2):
            state = (jnp.zeros((8, 128), F32), jnp.zeros((2, 128), F32))
            level = low
            kept, kept_level = jnp.zeros((2, 128), F32), low
            lines = [None] * NZ
            for n in range(NZ) if d == 0 else reversed(range(NZ)):
                lines[n] = state[0]
                kept = jnp.where(z == n, state[1], kept)
                kept_level = jnp.where(z == n, level, kept_level)
                piece = (rz[n].astype(F32)[8 * d : 8 * d + 8, :], rgs[n, 2 * d : 2 * d + 2, :])
                state, level = joined(state, level, piece, rgs[n, 5 + 2 * d : 6 + 2 * d, :], rgs[n, 4 + 2 * d : 5 + 2 * d, :])
            entering.append(lines)
            later["came"].append(kept)
            later["came_level"].append(kept_level)
        for n in range(NZ):
            iz[n] = jnp.concatenate([entering[0][n], entering[1][n]], axis=0).astype(BF16)
        ri[z] = iz[z]
        for dz in far_first:
            to = zat(dz)
            go(iz.at[to], ri.at[z], 10, step_r.at[4], {"z": to})

    plan(TZ, pieces_back)
    run()
    query.end()
    q[...] = jnp.dot(normed[...], w_q[...].reshape(D, 256), preferred_element_type=F32).astype(BF16)
    values.end()
    glu[...] = (project(w_glu, 0) * jax.nn.sigmoid(project(w_glu, 1))).astype(BF16)
    in_f_row, in_b_row = later["rows"]
    sum_f, sum_f_row, sum_b, sum_b_row = later["sums"]
    after = {"z": zat(lax.convert_element_type(y == NY - 1, jnp.int32)), "y": yat(1)}
    before = {"z": lax.rem(z + NZ - lax.convert_element_type(y == 0, jnp.int32), NZ), "y": yat(-1)}
    halos = [
        go(glu.at[pl.ds(240, 16), :], halo.at[0], 11, h_r.at[0], after),
        go(glu.at[pl.ds(0, 16), :], halo.at[1], 11, h_r.at[1], before),
    ]

    scores = lax.dot_general(q[...], k[...], (((1,), (1,)), ((), ())), preferred_element_type=F32) * 0.0625

    def inside(mask, sums, sum_row, gate_at, numerator):
        log_weight = jnp.where(mask, sums - sum_row + gate_at, NEG)
        top = jnp.max(log_weight, axis=1, keepdims=True)
        weights = scores * jnp.exp(log_weight - top)
        numerator[...] = jnp.dot(weights.astype(BF16), v[...], preferred_element_type=F32)
        return jnp.sum(weights, axis=1, keepdims=True), top

    den_f, top_f = inside(s_at <= t_at, sum_f, sum_f_row, in_f_row, num_f)

    all_of(ri.at[pl.ds(0, 15)], step_r.at[4])
    back = [None] * 2
    kept_vec = []
    for d in range(2):
        start = (ri[...].astype(F32)[:, 8 * d : 8 * d + 8, :], later["came"][d])
        found, _, _ = y_walk(d, start, later["came_level"][d])
        kept, kept_level = jnp.zeros((2, 128), F32), low
        back[d] = [None] * NY
        for n, state, level in found:
            back[d][n] = state[0]
            kept = jnp.where(y == n, state[1], kept)
            kept_level = jnp.where(y == n, level, kept_level)
        kept_vec.append((kept, kept_level))
    for n in range(NY):
        inc[n] = jnp.concatenate([back[0][n], back[1][n]], axis=1).astype(BF16)
    rin[y] = inc[y]
    for dy in (2, 1, 3):
        to = yat(dy)
        go(inc.at[to], rin.at[y], 9, step_r.at[5], {"y": to})
    for copy in halos:
        copy.wait_recv()
    place = z * NY + y
    for h in range(2):
        cols = slice(128 * h, 128 * h + 128)
        ext[h, 0:16, :] = jnp.where(place == 0, 0.0, halo[0][:, cols].astype(F32))
        ext[h, 16:272, :] = glu[:, cols].astype(F32)
        ext[h, 272:288, :] = jnp.where(place == NZ * NY - 1, 0.0, halo[1][:, cols].astype(F32))
    for h in range(2):
        cols = slice(128 * h, 128 * h + 128)

        def rows_of(n, carry):
            start = n * 64
            total = jnp.zeros((64, 128), F32)
            for j in range(31):
                total = total + taps[j : j + 1, cols] * ext[h, pl.ds(start + (j + 1), 64), :]
            cv[pl.ds(pl.multiple_of(start, 64), 64), cols] = total
            return carry

        lax.fori_loop(0, 4, rows_of, 0)
    conv = cv[...]
    stat[0:1, :] = as_row(jnp.sum(conv, axis=1, keepdims=True))
    stat[1:2, :] = as_row(jnp.sum(conv * conv, axis=1, keepdims=True))
    stat[2:8, :] = jnp.zeros((6, TOKENS), F32)
    tp_peers = [(dx, cc) for dx in range(NX) for cc in range(2) if dx or cc]
    for n, (dx, cc) in enumerate(tp_peers):
        dev = {"x": xat(dx), "c": core if cc == 0 else other}
        go(stat, rstat.at[n], 11, step_r.at[6], dev)
    den_b, top_b = inside(s_at >= t_at, sum_b, sum_b_row, in_b_row, num_b)

    all_of(rin.at[pl.ds(0, 3)], step_r.at[5])

    def finished(d, numerator, den, top, sums):
        vec, level = kept_vec[d]
        vec = jnp.concatenate([vec[0:1, :], vec[1:2, :]], axis=1)
        state = rin[...].reshape(64, 16, 128).astype(F32)[:, 8 * d : 8 * d + 8, :]
        left = state[:32].reshape(256, 128).astype(BF16)
        right = state[32:].reshape(256, 128).astype(BF16)
        carried = sums + level[:, 0:1]
        high = jnp.maximum(top, carried)
        near = jnp.exp(top - high)
        far = jnp.exp(carried - high)
        read = jnp.concatenate(
            [jnp.dot(q[...], left, preferred_element_type=F32), jnp.dot(q[...], right, preferred_element_type=F32)], axis=1
        )
        upper = near * numerator[...] + far * read
        lower = near * den + far * jnp.sum(q[...].astype(F32) * vec, axis=1, keepdims=True)
        return upper / jnp.maximum(jnp.abs(lower), jnp.exp(-high))

    summed = finished(0, num_f, den_f, top_f, sum_f) + finished(1, num_b, den_b, top_b, sum_b)
    scale = lax.rsqrt(jnp.mean(summed * summed, axis=1, keepdims=True) + EPS)
    heads = (summed * scale * mem_gain[...]).astype(BF16).reshape(4, 2, 32, 256)
    mem[0] = heads[:, 0]
    mem[1] = heads[:, 1]

    sums = stat[...]
    all_of(rstat, step_r.at[6])
    for n in range(7):
        sums = sums + rstat[n]
    mean = as_column(sums[0:1, :]) / CONV
    var = as_column(sums[1:2, :]) / CONV - mean * mean
    normal = (cv[...] - mean) * lax.rsqrt(var + EPS) * ln_gain[...] + ln_bias[...]
    gated = (normal * jax.nn.sigmoid(normal)).astype(BF16).reshape(4, 2, 32, 256)
    act[0] = gated[:, 0]
    act[1] = gated[:, 1]

    def part(c, h):
        cols = slice(1024 * h, 1024 * h + 1024)
        rows = jnp.dot(act[c].reshape(128, 256), wc[:, cols], preferred_element_type=F32)
        return (rows + jnp.dot(mem[c].reshape(128, 256), wm[:, cols], preferred_element_type=F32)).reshape(4, 32, 1024)

    d_in = []
    for h in range(2):
        psend[h] = part(other, h).astype(BF16)
        d_in.append(go(psend.at[h], precv.at[h], 7, d_r.at[h], {"c": other}))
    o_in = []
    for h in range(2):
        pair[...] = part(core, h)
        d_in[h].wait_recv()
        pair[...] = pair[...] + precv[h].astype(F32)
        sign = 1 - 2 * h
        xfar[h] = pair[xat(2)].astype(BF16)
        xnear[h] = pair[xat(-sign)].astype(BF16)
        far = go(xfar.at[h], rfar.at[h], 8, o_r.at[0, h], {"x": xat(sign)})
        near = go(xnear.at[h], rnear.at[h], 8, o_r.at[1, h], {"x": xat(-sign)})
        o_in.append((far, near))
        psum = pair[xat(sign)]
        rest = pair[x]
        if h == 0:
            held = psum, rest
    both = [held, (psum, rest)]
    last = []
    for h in range(2):
        sign = 1 - 2 * h
        o_in[h][0].wait_recv()
        xsum[h] = (both[h][0] + rfar[h].astype(F32)).astype(BF16)
        last.append(go(xsum.at[h], rsum.at[h], 8, o_r.at[2, h], {"x": xat(sign)}))
    for h in range(2):
        o_in[h][1].wait_recv()
        last[h].wait_recv()
        out[:, 1024 * h : 1024 * h + 1024] = (both[h][1] + rnear[h].astype(F32) + rsum[h].astype(F32)).astype(BF16)
    for n, size in enumerate(sent):
        if size > 1024 * 1024:
            count, same = size // 131072, w_kv
        elif size > 256 * 1024:
            count, same = size // 16384, w_q
        else:
            count, same = size // 4096, st
        assert size % count == 0
        all_of(same.at[pl.ds(0, count)], out_sem.at[n])


SP = ("z", "y")
TP = ("x", "c")


def shards(
    tokens, norm_gain, glu_value, glu_gate, conv_taps, ln_gain, ln_bias, query_weight, key_weight, value_weight,
    gate_weight, gate_bias, log_decay_extra, mem_gain, out_conv, out_mem,
):
    hbm = pl.BlockSpec(memory_space=pltpu.HBM)
    dma = pltpu.SemaphoreType.DMA
    V = pltpu.VMEM
    return pl.pallas_call(
        layer,
        out_shape=jax.ShapeDtypeStruct((32, D), BF16),
        in_specs=[hbm] * 16,
        out_specs=pl.BlockSpec(memory_space=pltpu.VMEM),
        scratch_shapes=[
            V((16, 4, ROWS, 512), BF16), V((16, 4, ROWS, 512), BF16), V((64, ROWS, 256), BF16),
            V((8, TOKENS, 256), BF16), V((TOKENS, D), BF16),
            V((1, D), F32), V((32, D), BF16), V((32, D), BF16), V((1, 32), F32), V((16, TOKENS), F32), V((31, 256), F32),
            V((1, 256), F32), V((1, 256), F32), V((1, 256), F32), V((256, D), BF16), V((256, D), BF16),
            V((TOKENS, 256), BF16), V((TOKENS, 256), BF16), V((TOKENS, 256), BF16), V((TOKENS, 256), BF16),
            V((64, 16, 128), BF16), V((8, 128), F32),
            V((4, 16, 16, 128), BF16), V((4, 8, 128), F32),
            V((16, 16, 128), BF16), V((8, 128), F32),
            V((16, 16, 128), BF16), V((16, 8, 128), F32),
            V((16, 16, 128), BF16), V((16, 16, 128), BF16),
            V((4, 16, 16, 128), BF16), V((4, 16, 16, 128), BF16),
            V((2, 16, 256), BF16), V((2, 288, 128), F32), V((256, 256), F32),
            V((8, 256), F32), V((7, 8, 256), F32),
            V((2, 4, 32, 256), BF16), V((2, 4, 32, 256), BF16),
            V((256, 256), F32), V((256, 256), F32),
            V((2, 4, 32, 1024), BF16), V((2, 4, 32, 1024), BF16),
            V((2, 32, 1024), BF16), V((2, 32, 1024), BF16), V((2, 32, 1024), BF16),
            V((2, 32, 1024), BF16), V((2, 32, 1024), BF16), V((2, 32, 1024), BF16),
            V((4, 32, 1024), F32),
            dma((16,)), dma((12,)),
            dma((2, 8)), dma((7, 4)), dma((2, 8)), dma((7, 4)), dma((4,)), dma((2, 8)),
            dma((4,)), dma((5,)), dma((2,)), dma((7,)), dma((2,)), dma((3, 2)),
        ],
        compiler_params=pltpu.CompilerParams(collective_id=0, has_side_effects=True, vmem_limit_bytes=VMEM_BYTES),
        name="layer",
    )(
        tokens, glu_value, glu_gate, query_weight, key_weight, value_weight,
        norm_gain.reshape(1, D), gate_weight.T, gate_bias.reshape(1, 32), log_decay_extra.T, conv_taps,
        ln_gain.reshape(1, 256), ln_bias.reshape(1, 256), mem_gain.reshape(1, 256), out_conv, out_mem,
    )


VMEM_BYTES = 60 * 1024 * 1024
HOP1, SIDE1, HOP2, SIDE2 = 2.3, 2.0, 3.2, 2.2
T2, TS, TY, TZ = 16.0, 26.0, 32.5, 41.0


def solution(mesh):
    split = Mesh(mesh.devices.reshape(NZ, NY, NX, 2), ("z", "y", "x", "c"))
    placed = (
        P(SP, TP), P(), P(SP, TP), P(SP, TP), P(None, TP), P(TP), P(TP), P(SP, TP), P(SP, TP), P(SP, TP),
        P(), P(), P(SP, None), P(TP), P(TP, None), P(TP, None),
    )
    return jax.shard_map(shards, mesh=split, in_specs=placed, out_specs=P(SP + TP, None), check_vma=False)
```

```python
import jax
import jax.numpy as jnp
from jax import lax
from jax.experimental import pallas as pl
from jax.experimental.pallas import tpu as pltpu
from jax.sharding import Mesh
from jax.sharding import PartitionSpec as P

MESH = pl.DeviceIdType.MESH
NZ, NY, NX = 16, 4, 4
ROWS = 32
TOKENS = 256
D = 2048
CONV = 2048
NEG = -1e30
EPS = 1e-06
F32 = jnp.float32
BF16 = jnp.bfloat16


def joined(state, level, new_state, new_level, decay):
    top = jnp.maximum(level + decay, new_level)
    early = jnp.exp(level + decay - top)
    late = jnp.exp(new_level - top)
    parts = []
    for old, new in zip(state, new_state):
        if old.ndim == 3:
            parts.append(early[None] * old + late[None] * new)
        else:
            parts.append(early * old + late * new)
    return tuple(parts), top


def log_sigmoid(x):
    return -(jnp.maximum(-x, 0.0) + jnp.log1p(jnp.exp(-jnp.abs(x))))


def ring(name, count):
    me = lax.axis_index(name)

    def at(step):
        return lax.rem(me + (step % count), count)

    return at


def remote(src, dst, ss, rs, dev):
    return pltpu.make_async_remote_copy(src, dst, ss, rs, device_id=dev, device_id_type=MESH)


SEED = 5
GROUPS = ((2, ((6, 5),)), (4, ((11, 4), (2, 4))), (8, ((15, 1), (0, 2))))


def step_of(sign, s):
    fresh = s in (1, SEED)
    return (8 if fresh else 8 + sign * (s - 1)), (8 + sign * s) % 16, s if fresh else 1


def time_of(s, hop, seed):
    return hop * s if s < SEED else seed + hop * (s - SEED)


class ZThenY:
    def __init__(self, plan, go, w, z_sem, y_sem, z_out, y_out, base, hop, seed, side):
        self.plan, self.go, self.w, self.seed = plan, go, w, seed
        self.z_sem, self.y_sem, self.z_out, self.y_out = z_sem, y_sem, z_out, y_out
        self.zat, self.yat = ring("z", NZ), ring("y", NY)
        self.y = lax.axis_index("y")
        self.base, self.hop, self.side = base, hop, side
        self.late = []
        self.count = 0

    def begin(self):
        for s in (SEED, 1):
            for way in range(2):
                self.along(way, s)

    def along(self, way, s):
        sign = 1 - 2 * way
        src, dst, away = step_of(sign, s)
        if s < 8:
            src, dst = self.w.at[src, self.y], self.w.at[dst, self.y]
        else:
            src, dst = self.w.at[src, self.y, pl.ds(16 * way, 16)], self.w.at[dst, self.y, pl.ds(16 * way, 16)]
        copy = self.go(src, dst, self.z_out, self.z_sem.at[way, s - 1], {"z": self.zat(sign * away)})
        now = self.base + time_of(s, self.hop, self.seed)

        def landed():
            copy.wait_recv()
            if s not in (SEED - 1, 8):
                self.along(way, s + 1)
            if way == 1:
                for last, ranges in GROUPS:
                    if last == s:
                        for first, count in ranges:
                            self.spread(first, count, now)

        self.plan(now, landed)

    def spread(self, first, count, now):
        n = self.count
        self.count += 1
        block = self.w.at[pl.ds(first, count), self.y]
        for way in range(2):
            sign = 1 - 2 * way
            copy = self.go(block, block, self.y_out, self.y_sem.at[n, way], {"y": self.yat(sign)})

            def landed(way=way, sign=sign, copy=copy):
                copy.wait_recv()
                half = self.w.at[pl.ds(first, count), self.yat(-sign), pl.ds(16 * way, 16)]
                self.late.append(self.go(half, half, self.y_out, self.y_sem.at[n, 2 + way], {"y": self.yat(sign)}))

            self.plan(now + self.side + 0.7 * count, landed)

    def end(self):
        for copy in self.late:
            copy.wait_recv()


class YThenZ:
    def __init__(self, plan, go, w, y_sem, z_sem, out, base, hop, seed, side):
        self.seed = seed
        self.plan, self.go, self.w, self.y_sem, self.z_sem, self.out = plan, go, w, y_sem, z_sem, out
        self.zat, self.yat = ring("z", NZ), ring("y", NY)
        self.base, self.hop, self.side = base, hop, side
        self.far, self.late = [], []

    def begin(self, now):
        block = self.w.at[32 + lax.axis_index("y")]
        for way in range(2):
            sign = 1 - 2 * way
            copy = self.go(block, block, self.out, self.y_sem.at[way], {"y": self.yat(sign)})

            def landed(way=way, sign=sign, copy=copy):
                copy.wait_recv()
                half = self.w.at[32 + self.yat(-sign), pl.ds(16 * way, 16)]
                self.far.append(self.go(half, half, self.out, self.y_sem.at[2 + way], {"y": self.yat(sign)}))

            self.plan(now + self.side, landed)

    def begin_z(self):
        for copy in self.far:
            copy.wait_recv()
        for s in (SEED, 1):
            for way in range(2):
                self.along(way, s)

    def along(self, way, s):
        sign = 1 - 2 * way
        src, dst, away = step_of(sign, s)
        if s < 8:
            src, dst = self.w.at[pl.ds(4 * src, 4)], self.w.at[pl.ds(4 * dst, 4)]
        else:
            src, dst = self.w.at[pl.ds(4 * src + 2 * way, 2)], self.w.at[pl.ds(4 * dst + 2 * way, 2)]
        copy = self.go(src, dst, self.out, self.z_sem.at[way, s - 1], {"z": self.zat(sign * away)})
        if s == 8:
            self.late.append(copy)
            return

        def landed():
            copy.wait_recv()
            self.along(way, s + 1)

        if s == SEED - 1:
            self.late.append(copy)
            return
        self.plan(self.base + time_of(s, self.hop, self.seed), landed)

    def end(self):
        for copy in self.late:
            copy.wait_recv()


def layer(
    tok, wv, wg, wq, wk, wl, gain_h, gate_h, bias_h, extra_h, taps_h, lng_h, lnb_h, memg_h, oc_h, om_h,
    out,
    w_kv, w_glu, w_q, rows_in, normed,
    gain, gate_w, gate_r, gate_b, extra, taps, ln_gain, ln_bias, mem_gain, wc, wm,
    glu, q, k, v,
    st, sm, ry, rsm, tz, gsm, rz, rgs, iz, ri, inc, rin,
    halo, ext, cv, stat, rstat, act, mem, num_f, num_b,
    psend, precv, xfar, xnear, xsum, rfar, rnear, rsum, pair,
    own, out_sem, kv_z, kv_y, glu_z, glu_y, q_y, q_z, tx_r, td_r, h_r, step_r, d_r, o_r,
):
    zat, yat, xat = ring("z", NZ), ring("y", NY), ring("x", NX)
    z, y, x, core = lax.axis_index("z"), lax.axis_index("y"), lax.axis_index("x"), lax.axis_index("c")
    other = 1 - core
    head = x * 2 + core
    sent = [0] * 12

    def go(src, dst, out_to, landed, dev):
        copy = remote(src, dst, out_sem.at[out_to], landed, dev)
        copy.start()
        size = 1
        for n in src.shape:
            size *= n
        sent[out_to] += size * jnp.dtype(src.dtype).itemsize
        return copy

    def all_of(ref, sem):
        pltpu.make_async_copy(ref, ref, sem).wait()

    def load(src, dst, n):
        copy = pltpu.make_async_copy(src, dst, own.at[n])
        copy.start()
        return copy

    l_kv = [load(src, w_kv.at[8, y, :, pl.ds(256 * n, 256)], n) for n, src in enumerate((wk, wl))]
    l_tok = load(tok, rows_in.at[head], 2)
    l_rest = [load(src, w_glu.at[8, y, :, pl.ds(256 * n, 256)], 3 + n) for n, src in enumerate((wv, wg))]
    l_q = load(wq, w_q.at[32 + y], 5)
    small = [(gain_h, gain), (gate_h, gate_w), (bias_h, gate_b), (extra_h, extra), (taps_h, taps), (lng_h, ln_gain),
             (lnb_h, ln_bias), (memg_h, mem_gain), (oc_h, wc), (om_h, wm)]
    small = [load(src, dst, 6 + n) for n, (src, dst) in enumerate(small)]

    barrier = pltpu.get_barrier_semaphore()
    greeted = [{"z": zat(1)}, {"z": zat(-1)}, {"z": zat(SEED)}, {"z": zat(-SEED)}, {"y": yat(1)}, {"y": yat(-1)}, {"x": xat(1)}, {"x": xat(-1)}, {"c": other}]
    for dev in greeted:
        pl.semaphore_signal(barrier, inc=1, device_id=dev, device_id_type=MESH)
    pl.semaphore_wait(barrier, len(greeted))

    tasks = []
    later = {}

    def plan(when, act_on):
        tasks.append((when, len(tasks), act_on))

    def run():
        while tasks:
            item = min(tasks, key=lambda t: t[:2])
            tasks.remove(item)
            item[2]()

    for copy in l_kv:
        copy.wait()
    kv = ZThenY(plan, go, w_kv, kv_z, kv_y, 0, 1, 0.0, HOP1, SEED1, SIDE1)
    kv.begin()
    values = ZThenY(plan, go, w_glu, glu_z, glu_y, 2, 3, T2, HOP2, SEED2, SIDE2)
    query = YThenZ(plan, go, w_q, q_y, q_z, 4, T2, HOP3, SEED3, SIDE2)

    def tokens_out():
        l_tok.wait()
        block = rows_in.at[head]
        later["tx"] = [go(block, block, 5, tx_r.at[w], {"x": xat(1 - 2 * w)}) for w in range(2)]
        later["td"] = [go(block, block, 5, td_r.at[0], {"c": other})]
        l_q.wait()
        query.begin(0.1)

    def tokens_on():
        later["tx2"] = []
        for w in range(2):
            later["tx"][w].wait_recv()
            sign = 1 - 2 * w
            slot = xat(-sign) * 2 + core
            half = rows_in.at[slot, pl.ds(128 * w, 128)]
            later["tx2"].append(go(half, half, 5, tx_r.at[2 + w], {"x": xat(sign)}))
            later["td"].append(go(rows_in.at[slot], rows_in.at[slot], 5, td_r.at[1 + w], {"c": other}))

    def tokens_far():
        slot = xat(2) * 2 + core
        for w in range(2):
            later["tx2"][w].wait_recv()
            half = rows_in.at[slot, pl.ds(128 * w, 128)]
            later["td"].append(go(half, half, 5, td_r.at[3 + w], {"c": other}))

    def tokens_in():
        for copy in later["td"]:
            copy.wait_recv()
        for copy in small:
            copy.wait()
        square = jnp.zeros((TOKENS, 256), F32)
        for b in range(8):
            wide = rows_in[b].astype(F32)
            square = square + wide * wide
        scale = lax.rsqrt(jnp.sum(square, axis=1, keepdims=True) / D + EPS)
        for p in range(16):
            at_z = zat(8 - p)
            cols = pl.ds(pl.multiple_of(at_z * 128, 128), 128)
            part = rows_in[at_z // 2, :, pl.ds(pl.multiple_of((at_z % 2) * 128, 128), 128)].astype(F32)
            normed[:, 128 * p : 128 * p + 128] = (part * scale * gain[:, cols]).astype(BF16)
            gate_r[:, 128 * p : 128 * p + 128] = gate_w[:, cols]

    plan(0.0, tokens_out)
    plan(3.5, tokens_on)
    plan(7.0, tokens_far)
    plan(10.1, tokens_in)

    sub = lax.broadcasted_iota(jnp.int32, (32, TOKENS), 0)
    sub16 = lax.broadcasted_iota(jnp.int32, (16, TOKENS), 0)
    t_at = lax.broadcasted_iota(jnp.int32, (TOKENS, TOKENS), 0)
    s_at = lax.broadcasted_iota(jnp.int32, (TOKENS, TOKENS), 1)

    def as_row(col):
        return jnp.sum(jnp.where(t_at == s_at, col, 0.0), axis=0, keepdims=True)

    def as_column(row):
        return jnp.sum(jnp.where(t_at == s_at, row, 0.0), axis=1, keepdims=True)

    def ends(total, sum_row, gate):
        to_end = total - sum_row + gate
        level = jnp.max(to_end, axis=1, keepdims=True)
        return as_column(jnp.exp(to_end - level) * 0.0625), level

    def gates_in():
        diagonal = lax.broadcasted_iota(jnp.int32, (32, 32), 0) == lax.broadcasted_iota(jnp.int32, (32, 32), 1)
        bias = jnp.sum(jnp.where(diagonal, gate_b[...], 0.0), axis=1, keepdims=True)
        gates = lax.dot_general(gate_r[...], normed[...], (((1,), (1,)), ((), ())), preferred_element_type=F32) + bias

        def gate_row(n):
            return jnp.sum(jnp.where(sub == 8 * n + head, gates, 0.0), axis=0, keepdims=True)

        def extra_row(n):
            return jnp.sum(jnp.where(sub16 == 8 * n + head, extra[...], 0.0), axis=0, keepdims=True)

        later["rows"] = gate_row(0), gate_row(2)
        lf_f = log_sigmoid(gate_row(1)) + extra_row(0)
        lf_b = log_sigmoid(gate_row(3)) + extra_row(1)
        sum_f = jnp.sum(jnp.where(s_at <= t_at, lf_f, 0.0), axis=1, keepdims=True)
        sum_b = jnp.sum(jnp.where(s_at >= t_at, lf_b, 0.0), axis=1, keepdims=True)
        sum_f_row, sum_b_row = as_row(sum_f), as_row(sum_b)
        later["sums"] = sum_f, sum_f_row, sum_b, sum_b_row
        total_f = jnp.sum(lf_f, axis=1, keepdims=True)
        total_b = jnp.sum(lf_b, axis=1, keepdims=True)
        end_f, level_f = ends(total_f, sum_f_row, later["rows"][0])
        end_b, level_b = ends(total_b, sum_b_row, later["rows"][1])
        later["ends"] = end_f, end_b
        for n, one in enumerate((total_f, level_f, total_b, level_b)):
            sm[4 + n : 5 + n, :] = jnp.broadcast_to(one, (1, 128))

    plan(12.1, gates_in)

    def rest_out():
        for copy in l_rest:
            copy.wait()
        values.begin()
        query.begin_z()

    plan(T2, rest_out)

    def project(w, n):
        return jnp.dot(normed[...], w[:, :, :, 256 * n : 256 * n + 256].reshape(D, 256), preferred_element_type=F32)

    def states_out():
        kv.end()
        v[...] = project(w_kv, 1).astype(BF16)
        keys = project(w_kv, 0).astype(BF16)
        k[...] = keys
        keys = keys.astype(F32)

        def summary(end):
            weighted = keys * end
            state = lax.dot_general(weighted.astype(BF16), v[...], (((0,), (0,)), ((), ())), preferred_element_type=F32)
            return state, jnp.sum(weighted, axis=0, keepdims=True)

        state_f, vec_f = summary(later["ends"][0])
        state_b, vec_b = summary(later["ends"][1])
        for h in range(2):
            cols = slice(128 * h, 128 * h + 128)
            both = jnp.concatenate([state_f[:, cols].reshape(32, 8, 128), state_b[:, cols].reshape(32, 8, 128)], axis=1)
            st[32 * h : 32 * h + 32] = both.astype(BF16)
        for n, row in enumerate((vec_f[:, :128], vec_f[:, 128:], vec_b[:, :128], vec_b[:, 128:])):
            sm[n : n + 1, :] = row
        ry[y] = st[pl.ds(y * 16, 16)]
        rsm[y] = sm[...]
        for dy in (2, 1, 3):
            to = yat(dy)
            go(sm, rsm.at[y], 6, step_r.at[0], {"y": to})
            go(st.at[pl.ds(to * 16, 16)], ry.at[y], 6, step_r.at[1], {"y": to})

    plan(TS, states_out)

    def y_pieces(n, d):
        return ry[n].astype(F32)[:, 8 * d : 8 * d + 8, :], rsm[n, 2 * d : 2 * d + 2, :]

    def y_scalars(n, d):
        return rsm[n, 5 + 2 * d : 6 + 2 * d, :], rsm[n, 4 + 2 * d : 5 + 2 * d, :]

    def y_walk(d, start, level):
        state = start
        found = []
        for n in range(NY) if d == 0 else reversed(range(NY)):
            found.append((n, state, level))
            state, level = joined(state, level, y_pieces(n, d), *y_scalars(n, d))
        return found, state, level

    low = jnp.full((1, 128), NEG, F32)
    far_first = (8, 7, 9, 6, 10, 5, 11, 4, 12, 3, 13, 2, 14, 1, 15)

    def groups_out():
        all_of(rsm.at[pl.ds(0, 3)], step_r.at[0])
        all_of(ry.at[pl.ds(0, 3)], step_r.at[1])
        zero = (jnp.zeros((16, 8, 128), F32), jnp.zeros((2, 128), F32))
        groups = []
        for d in range(2):
            _, group, level = y_walk(d, zero, low)
            groups.append(group)
            gsm[2 * d : 2 * d + 2, :] = group[1]
            decay = low * 0.0
            for n in range(NY):
                decay = decay + y_scalars(n, d)[1]
            gsm[4 + 2 * d : 5 + 2 * d, :] = decay
            gsm[5 + 2 * d : 6 + 2 * d, :] = level
        tz[...] = jnp.concatenate([groups[0][0], groups[1][0]], axis=1).astype(BF16)
        rz[z] = tz[z]
        rgs[z] = gsm[...]
        for dz in far_first:
            to = zat(dz)
            go(tz.at[to], rz.at[z], 10, step_r.at[2], {"z": to})
            go(gsm, rgs.at[z], 10, step_r.at[3], {"z": to})

    plan(TY, groups_out)

    def pieces_back():
        all_of(rz.at[pl.ds(0, 15)], step_r.at[2])
        all_of(rgs.at[pl.ds(0, 15)], step_r.at[3])
        later["came"], later["came_level"] = [], []
        entering = []
        for d in range(2):
            state = (jnp.zeros((8, 128), F32), jnp.zeros((2, 128), F32))
            level = low
            kept, kept_level = jnp.zeros((2, 128), F32), low
            lines = [None] * NZ
            for n in range(NZ) if d == 0 else reversed(range(NZ)):
                lines[n] = state[0]
                kept = jnp.where(z == n, state[1], kept)
                kept_level = jnp.where(z == n, level, kept_level)
                piece = (rz[n].astype(F32)[8 * d : 8 * d + 8, :], rgs[n, 2 * d : 2 * d + 2, :])
                state, level = joined(state, level, piece, rgs[n, 5 + 2 * d : 6 + 2 * d, :], rgs[n, 4 + 2 * d : 5 + 2 * d, :])
            entering.append(lines)
            later["came"].append(kept)
            later["came_level"].append(kept_level)
        for n in range(NZ):
            iz[n] = jnp.concatenate([entering[0][n], entering[1][n]], axis=0).astype(BF16)
        ri[z] = iz[z]
        for dz in far_first:
            to = zat(dz)
            go(iz.at[to], ri.at[z], 10, step_r.at[4], {"z": to})

    plan(TZ, pieces_back)
    run()
    query.end()
    q[...] = jnp.dot(normed[...], w_q[...].reshape(D, 256), preferred_element_type=F32).astype(BF16)
    values.end()
    glu[...] = (project(w_glu, 0) * jax.nn.sigmoid(project(w_glu, 1))).astype(BF16)
    in_f_row, in_b_row = later["rows"]
    sum_f, sum_f_row, sum_b, sum_b_row = later["sums"]
    after = {"z": zat(lax.convert_element_type(y == NY - 1, jnp.int32)), "y": yat(1)}
    before = {"z": lax.rem(z + NZ - lax.convert_element_type(y == 0, jnp.int32), NZ), "y": yat(-1)}
    halos = [
        go(glu.at[pl.ds(240, 16), :], halo.at[0], 11, h_r.at[0], after),
        go(glu.at[pl.ds(0, 16), :], halo.at[1], 11, h_r.at[1], before),
    ]

    scores = lax.dot_general(q[...], k[...], (((1,), (1,)), ((), ())), preferred_element_type=F32) * 0.0625

    def inside(mask, sums, sum_row, gate_at, numerator):
        log_weight = jnp.where(mask, sums - sum_row + gate_at, NEG)
        top = jnp.max(log_weight, axis=1, keepdims=True)
        weights = scores * jnp.exp(log_weight - top)
        numerator[...] = jnp.dot(weights.astype(BF16), v[...], preferred_element_type=F32)
        return jnp.sum(weights, axis=1, keepdims=True), top

    den_f, top_f = inside(s_at <= t_at, sum_f, sum_f_row, in_f_row, num_f)

    all_of(ri.at[pl.ds(0, 15)], step_r.at[4])
    back = [None] * 2
    kept_vec = []
    for d in range(2):
        start = (ri[...].astype(F32)[:, 8 * d : 8 * d + 8, :], later["came"][d])
        found, _, _ = y_walk(d, start, later["came_level"][d])
        kept, kept_level = jnp.zeros((2, 128), F32), low
        back[d] = [None] * NY
        for n, state, level in found:
            back[d][n] = state[0]
            kept = jnp.where(y == n, state[1], kept)
            kept_level = jnp.where(y == n, level, kept_level)
        kept_vec.append((kept, kept_level))
    for n in range(NY):
        inc[n] = jnp.concatenate([back[0][n], back[1][n]], axis=1).astype(BF16)
    rin[y] = inc[y]
    for dy in (2, 1, 3):
        to = yat(dy)
        go(inc.at[to], rin.at[y], 9, step_r.at[5], {"y": to})
    for copy in halos:
        copy.wait_recv()
    place = z * NY + y
    for h in range(2):
        cols = slice(128 * h, 128 * h + 128)
        ext[h, 0:16, :] = jnp.where(place == 0, 0.0, halo[0][:, cols].astype(F32))
        ext[h, 16:272, :] = glu[:, cols].astype(F32)
        ext[h, 272:288, :] = jnp.where(place == NZ * NY - 1, 0.0, halo[1][:, cols].astype(F32))
    for h in range(2):
        cols = slice(128 * h, 128 * h + 128)

        def rows_of(n, carry):
            start = n * 64
            total = jnp.zeros((64, 128), F32)
            for j in range(31):
                total = total + taps[j : j + 1, cols] * ext[h, pl.ds(start + (j + 1), 64), :]
            cv[pl.ds(pl.multiple_of(start, 64), 64), cols] = total
            return carry

        lax.fori_loop(0, 4, rows_of, 0)
    conv = cv[...]
    stat[0:1, :] = as_row(jnp.sum(conv, axis=1, keepdims=True))
    stat[1:2, :] = as_row(jnp.sum(conv * conv, axis=1, keepdims=True))
    stat[2:8, :] = jnp.zeros((6, TOKENS), F32)
    tp_peers = [(dx, cc) for dx in range(NX) for cc in range(2) if dx or cc]
    for n, (dx, cc) in enumerate(tp_peers):
        dev = {"x": xat(dx), "c": core if cc == 0 else other}
        go(stat, rstat.at[n], 11, step_r.at[6], dev)
    den_b, top_b = inside(s_at >= t_at, sum_b, sum_b_row, in_b_row, num_b)

    all_of(rin.at[pl.ds(0, 3)], step_r.at[5])

    def finished(d, numerator, den, top, sums):
        vec, level = kept_vec[d]
        vec = jnp.concatenate([vec[0:1, :], vec[1:2, :]], axis=1)
        state = rin[...].reshape(64, 16, 128).astype(F32)[:, 8 * d : 8 * d + 8, :]
        left = state[:32].reshape(256, 128).astype(BF16)
        right = state[32:].reshape(256, 128).astype(BF16)
        carried = sums + level[:, 0:1]
        high = jnp.maximum(top, carried)
        near = jnp.exp(top - high)
        far = jnp.exp(carried - high)
        read = jnp.concatenate(
            [jnp.dot(q[...], left, preferred_element_type=F32), jnp.dot(q[...], right, preferred_element_type=F32)], axis=1
        )
        upper = near * numerator[...] + far * read
        lower = near * den + far * jnp.sum(q[...].astype(F32) * vec, axis=1, keepdims=True)
        return upper / jnp.maximum(jnp.abs(lower), jnp.exp(-high))

    summed = finished(0, num_f, den_f, top_f, sum_f) + finished(1, num_b, den_b, top_b, sum_b)
    scale = lax.rsqrt(jnp.mean(summed * summed, axis=1, keepdims=True) + EPS)
    heads = (summed * scale * mem_gain[...]).astype(BF16).reshape(4, 2, 32, 256)
    mem[0] = heads[:, 0]
    mem[1] = heads[:, 1]

    sums = stat[...]
    all_of(rstat, step_r.at[6])
    for n in range(7):
        sums = sums + rstat[n]
    mean = as_column(sums[0:1, :]) / CONV
    var = as_column(sums[1:2, :]) / CONV - mean * mean
    normal = (cv[...] - mean) * lax.rsqrt(var + EPS) * ln_gain[...] + ln_bias[...]
    gated = (normal * jax.nn.sigmoid(normal)).astype(BF16).reshape(4, 2, 32, 256)
    act[0] = gated[:, 0]
    act[1] = gated[:, 1]

    def part(c, h):
        cols = slice(1024 * h, 1024 * h + 1024)
        rows = jnp.dot(act[c].reshape(128, 256), wc[:, cols], preferred_element_type=F32)
        return (rows + jnp.dot(mem[c].reshape(128, 256), wm[:, cols], preferred_element_type=F32)).reshape(4, 32, 1024)

    d_in = []
    for h in range(2):
        psend[h] = part(other, h).astype(BF16)
        d_in.append(go(psend.at[h], precv.at[h], 7, d_r.at[h], {"c": other}))
    o_in = []
    for h in range(2):
        pair[...] = part(core, h)
        d_in[h].wait_recv()
        pair[...] = pair[...] + precv[h].astype(F32)
        sign = 1 - 2 * h
        xfar[h] = pair[xat(2)].astype(BF16)
        xnear[h] = pair[xat(-sign)].astype(BF16)
        far = go(xfar.at[h], rfar.at[h], 8, o_r.at[0, h], {"x": xat(sign)})
        near = go(xnear.at[h], rnear.at[h], 8, o_r.at[1, h], {"x": xat(-sign)})
        o_in.append((far, near))
        psum = pair[xat(sign)]
        rest = pair[x]
        if h == 0:
            held = psum, rest
    both = [held, (psum, rest)]
    last = []
    for h in range(2):
        sign = 1 - 2 * h
        o_in[h][0].wait_recv()
        xsum[h] = (both[h][0] + rfar[h].astype(F32)).astype(BF16)
        last.append(go(xsum.at[h], rsum.at[h], 8, o_r.at[2, h], {"x": xat(sign)}))
    for h in range(2):
        o_in[h][1].wait_recv()
        last[h].wait_recv()
        out[:, 1024 * h : 1024 * h + 1024] = (both[h][1] + rnear[h].astype(F32) + rsum[h].astype(F32)).astype(BF16)
    for n, size in enumerate(sent):
        if size > 1024 * 1024:
            count, same = size // 131072, w_kv
        elif size > 256 * 1024:
            count, same = size // 16384, w_q
        else:
            count, same = size // 4096, st
        assert size % count == 0
        all_of(same.at[pl.ds(0, count)], out_sem.at[n])


SP = ("z", "y")
TP = ("x", "c")


def shards(
    tokens, norm_gain, glu_value, glu_gate, conv_taps, ln_gain, ln_bias, query_weight, key_weight, value_weight,
    gate_weight, gate_bias, log_decay_extra, mem_gain, out_conv, out_mem,
):
    hbm = pl.BlockSpec(memory_space=pltpu.HBM)
    dma = pltpu.SemaphoreType.DMA
    V = pltpu.VMEM
    return pl.pallas_call(
        layer,
        out_shape=jax.ShapeDtypeStruct((32, D), BF16),
        in_specs=[hbm] * 16,
        out_specs=pl.BlockSpec(memory_space=pltpu.VMEM),
        scratch_shapes=[
            V((16, 4, ROWS, 512), BF16), V((16, 4, ROWS, 512), BF16), V((64, ROWS, 256), BF16),
            V((8, TOKENS, 256), BF16), V((TOKENS, D), BF16),
            V((1, D), F32), V((32, D), BF16), V((32, D), BF16), V((1, 32), F32), V((16, TOKENS), F32), V((31, 256), F32),
            V((1, 256), F32), V((1, 256), F32), V((1, 256), F32), V((256, D), BF16), V((256, D), BF16),
            V((TOKENS, 256), BF16), V((TOKENS, 256), BF16), V((TOKENS, 256), BF16), V((TOKENS, 256), BF16),
            V((64, 16, 128), BF16), V((8, 128), F32),
            V((4, 16, 16, 128), BF16), V((4, 8, 128), F32),
            V((16, 16, 128), BF16), V((8, 128), F32),
            V((16, 16, 128), BF16), V((16, 8, 128), F32),
            V((16, 16, 128), BF16), V((16, 16, 128), BF16),
            V((4, 16, 16, 128), BF16), V((4, 16, 16, 128), BF16),
            V((2, 16, 256), BF16), V((2, 288, 128), F32), V((256, 256), F32),
            V((8, 256), F32), V((7, 8, 256), F32),
            V((2, 4, 32, 256), BF16), V((2, 4, 32, 256), BF16),
            V((256, 256), F32), V((256, 256), F32),
            V((2, 4, 32, 1024), BF16), V((2, 4, 32, 1024), BF16),
            V((2, 32, 1024), BF16), V((2, 32, 1024), BF16), V((2, 32, 1024), BF16),
            V((2, 32, 1024), BF16), V((2, 32, 1024), BF16), V((2, 32, 1024), BF16),
            V((4, 32, 1024), F32),
            dma((16,)), dma((12,)),
            dma((2, 8)), dma((5, 4)), dma((2, 8)), dma((5, 4)), dma((4,)), dma((2, 8)),
            dma((4,)), dma((5,)), dma((2,)), dma((7,)), dma((2,)), dma((3, 2)),
        ],
        compiler_params=pltpu.CompilerParams(collective_id=0, has_side_effects=True, vmem_limit_bytes=VMEM_BYTES),
        name="layer",
    )(
        tokens, glu_value, glu_gate, query_weight, key_weight, value_weight,
        norm_gain.reshape(1, D), gate_weight.T, gate_bias.reshape(1, 32), log_decay_extra.T, conv_taps,
        ln_gain.reshape(1, 256), ln_bias.reshape(1, 256), mem_gain.reshape(1, 256), out_conv, out_mem,
    )


VMEM_BYTES = 66700000
HOP1, SEED1, SIDE1 = 3.0, 6.1, 2.6
HOP2, SEED2, HOP3, SEED3, SIDE2 = 6.0, 10.0, 6.8, 11.0, 2.6
T2, TS, TY, TZ = 12.5, 27.5, 33.5, 41.5


def solution(mesh):
    split = Mesh(mesh.devices.reshape(NZ, NY, NX, 2), ("z", "y", "x", "c"))
    placed = (
        P(SP, TP), P(), P(SP, TP), P(SP, TP), P(None, TP), P(TP), P(TP), P(SP, TP), P(SP, TP), P(SP, TP),
        P(), P(), P(SP, None), P(TP), P(TP, None), P(TP, None),
    )
    return jax.shard_map(shards, mesh=split, in_specs=placed, out_specs=P(SP + TP, None), check_vma=False)
```

```python
import jax
import jax.numpy as jnp
from jax import lax
from jax.experimental import pallas as pl
from jax.experimental.pallas import tpu as pltpu
from jax.sharding import Mesh
from jax.sharding import PartitionSpec as P

MESH = pl.DeviceIdType.MESH
NZ, NY, NX = 16, 4, 4
ROWS = 32
TOKENS = 256
D = 2048
CONV = 2048
NEG = -1e30
EPS = 1e-06
F32 = jnp.float32
BF16 = jnp.bfloat16


def joined(state, level, new_state, new_level, decay):
    top = jnp.maximum(level + decay, new_level)
    early = jnp.exp(level + decay - top)
    late = jnp.exp(new_level - top)
    parts = []
    for old, new in zip(state, new_state):
        if old.ndim == 3:
            parts.append(early[None] * old + late[None] * new)
        else:
            parts.append(early * old + late * new)
    return tuple(parts), top


def log_sigmoid(x):
    return -(jnp.maximum(-x, 0.0) + jnp.log1p(jnp.exp(-jnp.abs(x))))


def ring(name, count):
    me = lax.axis_index(name)

    def at(step):
        return lax.rem(me + (step % count), count)

    return at


def remote(src, dst, ss, rs, dev):
    return pltpu.make_async_remote_copy(src, dst, ss, rs, device_id=dev, device_id_type=MESH)


SEED = 5
GROUPS = ((2, ((6, 5),)), (4, ((11, 4), (2, 4))), (8, ((15, 1), (0, 2))))


def step_of(sign, s):
    fresh = s in (1, SEED)
    return (8 if fresh else 8 + sign * (s - 1)), (8 + sign * s) % 16, s if fresh else 1


def time_of(s, hop, seed):
    return hop * s if s < SEED else seed + hop * (s - SEED)


class ZThenY:
    def __init__(self, plan, go, w, z_sem, y_sem, z_out, y_out, base, hop, seed, side):
        self.plan, self.go, self.w, self.seed = plan, go, w, seed
        self.z_sem, self.y_sem, self.z_out, self.y_out = z_sem, y_sem, z_out, y_out
        self.zat, self.yat = ring("z", NZ), ring("y", NY)
        self.y = lax.axis_index("y")
        self.base, self.hop, self.side = base, hop, side
        self.late = []
        self.count = 0

    def begin(self):
        for s in (SEED, 1):
            for way in range(2):
                self.along(way, s)

    def along(self, way, s):
        sign = 1 - 2 * way
        src, dst, away = step_of(sign, s)
        if s < 8:
            src, dst = self.w.at[src, self.y], self.w.at[dst, self.y]
        else:
            src, dst = self.w.at[src, self.y, pl.ds(16 * way, 16)], self.w.at[dst, self.y, pl.ds(16 * way, 16)]
        copy = self.go(src, dst, self.z_out, self.z_sem.at[way, s - 1], {"z": self.zat(sign * away)})
        now = self.base + time_of(s, self.hop, self.seed)

        def landed():
            copy.wait_recv()
            if s not in (SEED - 1, 8):
                self.along(way, s + 1)
            if way == 1:
                for last, ranges in GROUPS:
                    if last == s:
                        for first, count in ranges:
                            self.spread(first, count, now)

        self.plan(now, landed)

    def spread(self, first, count, now):
        n = self.count
        self.count += 1
        block = self.w.at[pl.ds(first, count), self.y]
        for way in range(2):
            sign = 1 - 2 * way
            copy = self.go(block, block, self.y_out, self.y_sem.at[n, way], {"y": self.yat(sign)})

            def landed(way=way, sign=sign, copy=copy):
                copy.wait_recv()
                half = self.w.at[pl.ds(first, count), self.yat(-sign), pl.ds(16 * way, 16)]
                self.late.append(self.go(half, half, self.y_out, self.y_sem.at[n, 2 + way], {"y": self.yat(sign)}))

            self.plan(now + self.side + 0.7 * count, landed)

    def end(self):
        for copy in self.late:
            copy.wait_recv()


class YThenZ:
    def __init__(self, plan, go, w, y_sem, z_sem, out, base, hop, seed, side):
        self.seed = seed
        self.plan, self.go, self.w, self.y_sem, self.z_sem, self.out = plan, go, w, y_sem, z_sem, out
        self.zat, self.yat = ring("z", NZ), ring("y", NY)
        self.base, self.hop, self.side = base, hop, side
        self.far, self.late = [], []

    def begin(self, now):
        block = self.w.at[32 + lax.axis_index("y")]
        for way in range(2):
            sign = 1 - 2 * way
            copy = self.go(block, block, self.out, self.y_sem.at[way], {"y": self.yat(sign)})

            def landed(way=way, sign=sign, copy=copy):
                copy.wait_recv()
                half = self.w.at[32 + self.yat(-sign), pl.ds(16 * way, 16)]
                self.far.append(self.go(half, half, self.out, self.y_sem.at[2 + way], {"y": self.yat(sign)}))

            self.plan(now + self.side, landed)

    def begin_z(self):
        for copy in self.far:
            copy.wait_recv()
        for s in (SEED, 1):
            for way in range(2):
                self.along(way, s)

    def along(self, way, s):
        sign = 1 - 2 * way
        src, dst, away = step_of(sign, s)
        if s < 8:
            src, dst = self.w.at[pl.ds(4 * src, 4)], self.w.at[pl.ds(4 * dst, 4)]
        else:
            src, dst = self.w.at[pl.ds(4 * src + 2 * way, 2)], self.w.at[pl.ds(4 * dst + 2 * way, 2)]
        copy = self.go(src, dst, self.out, self.z_sem.at[way, s - 1], {"z": self.zat(sign * away)})
        if s == 8:
            self.late.append(copy)
            return

        def landed():
            copy.wait_recv()
            self.along(way, s + 1)

        if s == SEED - 1:
            self.late.append(copy)
            return
        self.plan(self.base + time_of(s, self.hop, self.seed), landed)

    def end(self):
        for copy in self.late:
            copy.wait_recv()


def layer(
    tok, wv, wg, wq, wk, wl, gain_h, gate_h, bias_h, extra_h, taps_h, lng_h, lnb_h, memg_h, oc_h, om_h,
    out,
    w_kv, w_glu, w_q, rows_in, normed,
    gain, gate_w, gate_r, gate_b, extra, taps, ln_gain, ln_bias, mem_gain, wc, wm,
    glu, q, k, v,
    st, sm, ry, rsm, tz, gsm, rz, rgs, iz, ri, inc, rin,
    halo, ext, cv, stat, rstat, act, mem, num_f, num_b,
    psend, precv, xfar, xnear, xsum, rfar, rnear, rsum, pair,
    own, out_sem, kv_z, kv_y, glu_z, glu_y, q_y, q_z, tx_r, td_r, h_r, step_r, d_r, o_r,
):
    zat, yat, xat = ring("z", NZ), ring("y", NY), ring("x", NX)
    z, y, x, core = lax.axis_index("z"), lax.axis_index("y"), lax.axis_index("x"), lax.axis_index("c")
    other = 1 - core
    head = x * 2 + core
    sent = [0] * 12

    def go(src, dst, out_to, landed, dev):
        copy = remote(src, dst, out_sem.at[out_to], landed, dev)
        copy.start()
        size = 1
        for n in src.shape:
            size *= n
        sent[out_to] += size * jnp.dtype(src.dtype).itemsize
        return copy

    def all_of(ref, sem):
        pltpu.make_async_copy(ref, ref, sem).wait()

    def load(src, dst, n):
        copy = pltpu.make_async_copy(src, dst, own.at[n])
        copy.start()
        return copy

    l_kv = [load(src, w_kv.at[8, y, :, pl.ds(256 * n, 256)], n) for n, src in enumerate((wk, wl))]
    l_tok = load(tok, rows_in.at[head], 2)
    l_rest = [load(src, w_glu.at[8, y, :, pl.ds(256 * n, 256)], 3 + n) for n, src in enumerate((wv, wg))]
    l_q = load(wq, w_q.at[32 + y], 5)
    small = [(gain_h, gain), (gate_h, gate_w), (bias_h, gate_b), (extra_h, extra), (taps_h, taps), (lng_h, ln_gain),
             (lnb_h, ln_bias), (memg_h, mem_gain), (oc_h, wc), (om_h, wm)]
    small = [load(src, dst, 6 + n) for n, (src, dst) in enumerate(small)]

    barrier = pltpu.get_barrier_semaphore()
    greeted = [{"z": zat(1)}, {"z": zat(-1)}, {"z": zat(SEED)}, {"z": zat(-SEED)}, {"y": yat(1)}, {"y": yat(-1)}, {"x": xat(1)}, {"x": xat(-1)}, {"c": other}]
    for dev in greeted:
        pl.semaphore_signal(barrier, inc=1, device_id=dev, device_id_type=MESH)
    pl.semaphore_wait(barrier, len(greeted))

    tasks = []
    later = {}

    def plan(when, act_on):
        tasks.append((when, len(tasks), act_on))

    def run():
        while tasks:
            item = min(tasks, key=lambda t: t[:2])
            tasks.remove(item)
            item[2]()

    for copy in l_kv:
        copy.wait()
    kv = ZThenY(plan, go, w_kv, kv_z, kv_y, 0, 1, 0.0, HOP1, SEED1, SIDE1)
    kv.begin()
    values = ZThenY(plan, go, w_glu, glu_z, glu_y, 2, 3, T2, HOP2, SEED2, SIDE2)
    query = YThenZ(plan, go, w_q, q_y, q_z, 4, T2, HOP3, SEED3, SIDE2)

    def tokens_out():
        l_tok.wait()
        block = rows_in.at[head]
        later["tx"] = [go(block, block, 5, tx_r.at[w], {"x": xat(1 - 2 * w)}) for w in range(2)]
        later["td"] = [go(block, block, 5, td_r.at[0], {"c": other})]
        l_q.wait()
        query.begin(0.1)

    def tokens_on():
        later["tx2"] = []
        for w in range(2):
            later["tx"][w].wait_recv()
            sign = 1 - 2 * w
            slot = xat(-sign) * 2 + core
            half = rows_in.at[slot, pl.ds(128 * w, 128)]
            later["tx2"].append(go(half, half, 5, tx_r.at[2 + w], {"x": xat(sign)}))
            later["td"].append(go(rows_in.at[slot], rows_in.at[slot], 5, td_r.at[1 + w], {"c": other}))

    def tokens_far():
        slot = xat(2) * 2 + core
        for w in range(2):
            later["tx2"][w].wait_recv()
            half = rows_in.at[slot, pl.ds(128 * w, 128)]
            later["td"].append(go(half, half, 5, td_r.at[3 + w], {"c": other}))

    def tokens_in():
        for copy in later["td"]:
            copy.wait_recv()
        for copy in small:
            copy.wait()
        square = jnp.zeros((TOKENS, 256), F32)
        for b in range(8):
            wide = rows_in[b].astype(F32)
            square = square + wide * wide
        scale = lax.rsqrt(jnp.sum(square, axis=1, keepdims=True) / D + EPS)
        for p in range(16):
            at_z = zat(8 - p)
            cols = pl.ds(pl.multiple_of(at_z * 128, 128), 128)
            part = rows_in[at_z // 2, :, pl.ds(pl.multiple_of((at_z % 2) * 128, 128), 128)].astype(F32)
            normed[:, 128 * p : 128 * p + 128] = (part * scale * gain[:, cols]).astype(BF16)
            gate_r[:, 128 * p : 128 * p + 128] = gate_w[:, cols]

    plan(0.0, tokens_out)
    plan(3.5, tokens_on)
    plan(7.0, tokens_far)
    plan(10.1, tokens_in)

    sub = lax.broadcasted_iota(jnp.int32, (32, TOKENS), 0)
    sub16 = lax.broadcasted_iota(jnp.int32, (16, TOKENS), 0)
    t_at = lax.broadcasted_iota(jnp.int32, (TOKENS, TOKENS), 0)
    s_at = lax.broadcasted_iota(jnp.int32, (TOKENS, TOKENS), 1)

    def as_row(col):
        return jnp.sum(jnp.where(t_at == s_at, col, 0.0), axis=0, keepdims=True)

    def as_column(row):
        return jnp.sum(jnp.where(t_at == s_at, row, 0.0), axis=1, keepdims=True)

    def ends(total, sum_row, gate):
        to_end = total - sum_row + gate
        level = jnp.max(to_end, axis=1, keepdims=True)
        return as_column(jnp.exp(to_end - level) * 0.0625), level

    def gates_in():
        diagonal = lax.broadcasted_iota(jnp.int32, (32, 32), 0) == lax.broadcasted_iota(jnp.int32, (32, 32), 1)
        bias = jnp.sum(jnp.where(diagonal, gate_b[...], 0.0), axis=1, keepdims=True)
        gates = lax.dot_general(gate_r[...], normed[...], (((1,), (1,)), ((), ())), preferred_element_type=F32) + bias

        def gate_row(n):
            return jnp.sum(jnp.where(sub == 8 * n + head, gates, 0.0), axis=0, keepdims=True)

        def extra_row(n):
            return jnp.sum(jnp.where(sub16 == 8 * n + head, extra[...], 0.0), axis=0, keepdims=True)

        later["rows"] = gate_row(0), gate_row(2)
        lf_f = log_sigmoid(gate_row(1)) + extra_row(0)
        lf_b = log_sigmoid(gate_row(3)) + extra_row(1)
        sum_f = jnp.sum(jnp.where(s_at <= t_at, lf_f, 0.0), axis=1, keepdims=True)
        sum_b = jnp.sum(jnp.where(s_at >= t_at, lf_b, 0.0), axis=1, keepdims=True)
        sum_f_row, sum_b_row = as_row(sum_f), as_row(sum_b)
        later["sums"] = sum_f, sum_f_row, sum_b, sum_b_row
        total_f = jnp.sum(lf_f, axis=1, keepdims=True)
        total_b = jnp.sum(lf_b, axis=1, keepdims=True)
        end_f, level_f = ends(total_f, sum_f_row, later["rows"][0])
        end_b, level_b = ends(total_b, sum_b_row, later["rows"][1])
        later["ends"] = end_f, end_b
        for n, one in enumerate((total_f, level_f, total_b, level_b)):
            sm[4 + n : 5 + n, :] = jnp.broadcast_to(one, (1, 128))

    plan(12.6, gates_in)

    def rest_out():
        for copy in l_rest:
            copy.wait()
        values.begin()
        query.begin_z()

    plan(T2, rest_out)

    def project(w, n):
        return jnp.dot(normed[...], w[:, :, :, 256 * n : 256 * n + 256].reshape(D, 256), preferred_element_type=F32)

    def states_out():
        kv.end()
        v[...] = project(w_kv, 1).astype(BF16)
        keys = project(w_kv, 0).astype(BF16)
        k[...] = keys
        keys = keys.astype(F32)

        def summary(end):
            weighted = keys * end
            state = lax.dot_general(weighted.astype(BF16), v[...], (((0,), (0,)), ((), ())), preferred_element_type=F32)
            return state, jnp.sum(weighted, axis=0, keepdims=True)

        state_f, vec_f = summary(later["ends"][0])
        state_b, vec_b = summary(later["ends"][1])
        for h in range(2):
            cols = slice(128 * h, 128 * h + 128)
            both = jnp.concatenate([state_f[:, cols].reshape(32, 8, 128), state_b[:, cols].reshape(32, 8, 128)], axis=1)
            st[32 * h : 32 * h + 32] = both.astype(BF16)
        for n, row in enumerate((vec_f[:, :128], vec_f[:, 128:], vec_b[:, :128], vec_b[:, 128:])):
            sm[n : n + 1, :] = row
        ry[y] = st[pl.ds(y * 16, 16)]
        rsm[y] = sm[...]
        for dy in (2, 1, 3):
            to = yat(dy)
            go(sm, rsm.at[y], 6, step_r.at[0], {"y": to})
            go(st.at[pl.ds(to * 16, 16)], ry.at[y], 6, step_r.at[1], {"y": to})

    plan(TS, states_out)

    def y_pieces(n, d):
        return ry[n].astype(F32)[:, 8 * d : 8 * d + 8, :], rsm[n, 2 * d : 2 * d + 2, :]

    def y_scalars(n, d):
        return rsm[n, 5 + 2 * d : 6 + 2 * d, :], rsm[n, 4 + 2 * d : 5 + 2 * d, :]

    def y_walk(d, start, level):
        state = start
        found = []
        for n in range(NY) if d == 0 else reversed(range(NY)):
            found.append((n, state, level))
            state, level = joined(state, level, y_pieces(n, d), *y_scalars(n, d))
        return found, state, level

    low = jnp.full((1, 128), NEG, F32)
    far_first = (8, 7, 9, 6, 10, 5, 11, 4, 12, 3, 13, 2, 14, 1, 15)

    def groups_out():
        all_of(rsm.at[pl.ds(0, 3)], step_r.at[0])
        all_of(ry.at[pl.ds(0, 3)], step_r.at[1])
        zero = (jnp.zeros((16, 8, 128), F32), jnp.zeros((2, 128), F32))
        groups = []
        for d in range(2):
            _, group, level = y_walk(d, zero, low)
            groups.append(group)
            gsm[2 * d : 2 * d + 2, :] = group[1]
            decay = low * 0.0
            for n in range(NY):
                decay = decay + y_scalars(n, d)[1]
            gsm[4 + 2 * d : 5 + 2 * d, :] = decay
            gsm[5 + 2 * d : 6 + 2 * d, :] = level
        tz[...] = jnp.concatenate([groups[0][0], groups[1][0]], axis=1).astype(BF16)
        rz[z] = tz[z]
        rgs[z] = gsm[...]
        for dz in far_first:
            to = zat(dz)
            go(tz.at[to], rz.at[z], 10, step_r.at[2], {"z": to})
            go(gsm, rgs.at[z], 10, step_r.at[3], {"z": to})

    plan(TY, groups_out)

    def pieces_back():
        all_of(rz.at[pl.ds(0, 15)], step_r.at[2])
        all_of(rgs.at[pl.ds(0, 15)], step_r.at[3])
        later["came"], later["came_level"] = [], []
        entering = []
        for d in range(2):
            state = (jnp.zeros((8, 128), F32), jnp.zeros((2, 128), F32))
            level = low
            kept, kept_level = jnp.zeros((2, 128), F32), low
            lines = [None] * NZ
            for n in range(NZ) if d == 0 else reversed(range(NZ)):
                lines[n] = state[0]
                kept = jnp.where(z == n, state[1], kept)
                kept_level = jnp.where(z == n, level, kept_level)
                piece = (rz[n].astype(F32)[8 * d : 8 * d + 8, :], rgs[n, 2 * d : 2 * d + 2, :])
                state, level = joined(state, level, piece, rgs[n, 5 + 2 * d : 6 + 2 * d, :], rgs[n, 4 + 2 * d : 5 + 2 * d, :])
            entering.append(lines)
            later["came"].append(kept)
            later["came_level"].append(kept_level)
        for n in range(NZ):
            iz[n] = jnp.concatenate([entering[0][n], entering[1][n]], axis=0).astype(BF16)
        ri[z] = iz[z]
        for dz in far_first:
            to = zat(dz)
            go(iz.at[to], ri.at[z], 10, step_r.at[4], {"z": to})

    plan(TZ, pieces_back)
    run()
    query.end()
    q[...] = jnp.dot(normed[...], w_q[...].reshape(D, 256), preferred_element_type=F32).astype(BF16)
    values.end()
    glu[...] = (project(w_glu, 0) * jax.nn.sigmoid(project(w_glu, 1))).astype(BF16)
    in_f_row, in_b_row = later["rows"]
    sum_f, sum_f_row, sum_b, sum_b_row = later["sums"]
    after = {"z": zat(lax.convert_element_type(y == NY - 1, jnp.int32)), "y": yat(1)}
    before = {"z": lax.rem(z + NZ - lax.convert_element_type(y == 0, jnp.int32), NZ), "y": yat(-1)}
    halos = [
        go(glu.at[pl.ds(240, 16), :], halo.at[0], 11, h_r.at[0], after),
        go(glu.at[pl.ds(0, 16), :], halo.at[1], 11, h_r.at[1], before),
    ]

    scores = lax.dot_general(q[...], k[...], (((1,), (1,)), ((), ())), preferred_element_type=F32) * 0.0625

    def inside(mask, sums, sum_row, gate_at, numerator):
        log_weight = jnp.where(mask, sums - sum_row + gate_at, NEG)
        top = jnp.max(log_weight, axis=1, keepdims=True)
        weights = scores * jnp.exp(log_weight - top)
        numerator[...] = jnp.dot(weights.astype(BF16), v[...], preferred_element_type=F32)
        return jnp.sum(weights, axis=1, keepdims=True), top

    den_f, top_f = inside(s_at <= t_at, sum_f, sum_f_row, in_f_row, num_f)

    all_of(ri.at[pl.ds(0, 15)], step_r.at[4])
    back = [None] * 2
    kept_vec = []
    for d in range(2):
        start = (ri[...].astype(F32)[:, 8 * d : 8 * d + 8, :], later["came"][d])
        found, _, _ = y_walk(d, start, later["came_level"][d])
        kept, kept_level = jnp.zeros((2, 128), F32), low
        back[d] = [None] * NY
        for n, state, level in found:
            back[d][n] = state[0]
            kept = jnp.where(y == n, state[1], kept)
            kept_level = jnp.where(y == n, level, kept_level)
        kept_vec.append((kept, kept_level))
    for n in range(NY):
        inc[n] = jnp.concatenate([back[0][n], back[1][n]], axis=1).astype(BF16)
    rin[y] = inc[y]
    for dy in (2, 1, 3):
        to = yat(dy)
        go(inc.at[to], rin.at[y], 9, step_r.at[5], {"y": to})
    for copy in halos:
        copy.wait_recv()
    place = z * NY + y
    for h in range(2):
        cols = slice(128 * h, 128 * h + 128)
        ext[h, 0:16, :] = jnp.where(place == 0, 0.0, halo[0][:, cols].astype(F32))
        ext[h, 16:272, :] = glu[:, cols].astype(F32)
        ext[h, 272:288, :] = jnp.where(place == NZ * NY - 1, 0.0, halo[1][:, cols].astype(F32))
    for h in range(2):
        cols = slice(128 * h, 128 * h + 128)

        def rows_of(n, carry):
            start = n * 64
            total = jnp.zeros((64, 128), F32)
            for j in range(31):
                total = total + taps[j : j + 1, cols] * ext[h, pl.ds(start + (j + 1), 64), :]
            cv[pl.ds(pl.multiple_of(start, 64), 64), cols] = total
            return carry

        lax.fori_loop(0, 4, rows_of, 0)
    conv = cv[...]
    stat[0:1, :] = as_row(jnp.sum(conv, axis=1, keepdims=True))
    stat[1:2, :] = as_row(jnp.sum(conv * conv, axis=1, keepdims=True))
    stat[2:8, :] = jnp.zeros((6, TOKENS), F32)
    tp_peers = [(dx, cc) for dx in range(NX) for cc in range(2) if dx or cc]
    for n, (dx, cc) in enumerate(tp_peers):
        dev = {"x": xat(dx), "c": core if cc == 0 else other}
        go(stat, rstat.at[n], 11, step_r.at[6], dev)
    den_b, top_b = inside(s_at >= t_at, sum_b, sum_b_row, in_b_row, num_b)

    all_of(rin.at[pl.ds(0, 3)], step_r.at[5])

    def finished(d, numerator, den, top, sums):
        vec, level = kept_vec[d]
        vec = jnp.concatenate([vec[0:1, :], vec[1:2, :]], axis=1)
        state = rin[...].reshape(64, 16, 128).astype(F32)[:, 8 * d : 8 * d + 8, :]
        left = state[:32].reshape(256, 128).astype(BF16)
        right = state[32:].reshape(256, 128).astype(BF16)
        carried = sums + level[:, 0:1]
        high = jnp.maximum(top, carried)
        near = jnp.exp(top - high)
        far = jnp.exp(carried - high)
        read = jnp.concatenate(
            [jnp.dot(q[...], left, preferred_element_type=F32), jnp.dot(q[...], right, preferred_element_type=F32)], axis=1
        )
        upper = near * numerator[...] + far * read
        lower = near * den + far * jnp.sum(q[...].astype(F32) * vec, axis=1, keepdims=True)
        return upper / jnp.maximum(jnp.abs(lower), jnp.exp(-high))

    summed = finished(0, num_f, den_f, top_f, sum_f) + finished(1, num_b, den_b, top_b, sum_b)
    scale = lax.rsqrt(jnp.mean(summed * summed, axis=1, keepdims=True) + EPS)
    heads = (summed * scale * mem_gain[...]).astype(BF16).reshape(4, 2, 32, 256)
    mem[0] = heads[:, 0]
    mem[1] = heads[:, 1]

    sums = stat[...]
    all_of(rstat, step_r.at[6])
    for n in range(7):
        sums = sums + rstat[n]
    mean = as_column(sums[0:1, :]) / CONV
    var = as_column(sums[1:2, :]) / CONV - mean * mean
    normal = (cv[...] - mean) * lax.rsqrt(var + EPS) * ln_gain[...] + ln_bias[...]
    gated = (normal * jax.nn.sigmoid(normal)).astype(BF16).reshape(4, 2, 32, 256)
    act[0] = gated[:, 0]
    act[1] = gated[:, 1]

    def part(c, h):
        cols = slice(1024 * h, 1024 * h + 1024)
        rows = jnp.dot(act[c].reshape(128, 256), wc[:, cols], preferred_element_type=F32)
        return (rows + jnp.dot(mem[c].reshape(128, 256), wm[:, cols], preferred_element_type=F32)).reshape(4, 32, 1024)

    d_in = []
    for h in range(2):
        psend[h] = part(other, h).astype(BF16)
        d_in.append(go(psend.at[h], precv.at[h], 7, d_r.at[h], {"c": other}))
    o_in = []
    for h in range(2):
        pair[...] = part(core, h)
        d_in[h].wait_recv()
        pair[...] = pair[...] + precv[h].astype(F32)
        sign = 1 - 2 * h
        xfar[h] = pair[xat(2)].astype(BF16)
        xnear[h] = pair[xat(-sign)].astype(BF16)
        far = go(xfar.at[h], rfar.at[h], 8, o_r.at[0, h], {"x": xat(sign)})
        o_in.append(far)
        psum = pair[xat(sign)]
        rest = pair[x]
        if h == 0:
            held = psum, rest
    both = [held, (psum, rest)]
    near = [go(xnear.at[h], rnear.at[h], 8, o_r.at[1, h], {"x": xat(2 * h - 1)}) for h in range(2)]
    last = []
    for h in range(2):
        sign = 1 - 2 * h
        o_in[h].wait_recv()
        xsum[h] = (both[h][0] + rfar[h].astype(F32)).astype(BF16)
        last.append(go(xsum.at[h], rsum.at[h], 8, o_r.at[2, h], {"x": xat(sign)}))
    for h in range(2):
        near[h].wait_recv()
        last[h].wait_recv()
        out[:, 1024 * h : 1024 * h + 1024] = (both[h][1] + rnear[h].astype(F32) + rsum[h].astype(F32)).astype(BF16)
    for n, size in enumerate(sent):
        if size > 1024 * 1024:
            count, same = size // 131072, w_kv
        elif size > 256 * 1024:
            count, same = size // 16384, w_q
        else:
            count, same = size // 4096, st
        assert size % count == 0
        all_of(same.at[pl.ds(0, count)], out_sem.at[n])


SP = ("z", "y")
TP = ("x", "c")


def shards(
    tokens, norm_gain, glu_value, glu_gate, conv_taps, ln_gain, ln_bias, query_weight, key_weight, value_weight,
    gate_weight, gate_bias, log_decay_extra, mem_gain, out_conv, out_mem,
):
    hbm = pl.BlockSpec(memory_space=pltpu.HBM)
    dma = pltpu.SemaphoreType.DMA
    V = pltpu.VMEM
    return pl.pallas_call(
        layer,
        out_shape=jax.ShapeDtypeStruct((32, D), BF16),
        in_specs=[hbm] * 16,
        out_specs=pl.BlockSpec(memory_space=pltpu.VMEM),
        scratch_shapes=[
            V((16, 4, ROWS, 512), BF16), V((16, 4, ROWS, 512), BF16), V((64, ROWS, 256), BF16),
            V((8, TOKENS, 256), BF16), V((TOKENS, D), BF16),
            V((1, D), F32), V((32, D), BF16), V((32, D), BF16), V((1, 32), F32), V((16, TOKENS), F32), V((31, 256), F32),
            V((1, 256), F32), V((1, 256), F32), V((1, 256), F32), V((256, D), BF16), V((256, D), BF16),
            V((TOKENS, 256), BF16), V((TOKENS, 256), BF16), V((TOKENS, 256), BF16), V((TOKENS, 256), BF16),
            V((64, 16, 128), BF16), V((8, 128), F32),
            V((4, 16, 16, 128), BF16), V((4, 8, 128), F32),
            V((16, 16, 128), BF16), V((8, 128), F32),
            V((16, 16, 128), BF16), V((16, 8, 128), F32),
            V((16, 16, 128), BF16), V((16, 16, 128), BF16),
            V((4, 16, 16, 128), BF16), V((4, 16, 16, 128), BF16),
            V((2, 16, 256), BF16), V((2, 288, 128), F32), V((256, 256), F32),
            V((8, 256), F32), V((7, 8, 256), F32),
            V((2, 4, 32, 256), BF16), V((2, 4, 32, 256), BF16),
            V((256, 256), F32), V((256, 256), F32),
            V((2, 4, 32, 1024), BF16), V((2, 4, 32, 1024), BF16),
            V((2, 32, 1024), BF16), V((2, 32, 1024), BF16), V((2, 32, 1024), BF16),
            V((2, 32, 1024), BF16), V((2, 32, 1024), BF16), V((2, 32, 1024), BF16),
            V((4, 32, 1024), F32),
            dma((16,)), dma((12,)),
            dma((2, 8)), dma((5, 4)), dma((2, 8)), dma((5, 4)), dma((4,)), dma((2, 8)),
            dma((4,)), dma((5,)), dma((2,)), dma((7,)), dma((2,)), dma((3, 2)),
        ],
        compiler_params=pltpu.CompilerParams(collective_id=0, has_side_effects=True, vmem_limit_bytes=VMEM_BYTES),
        name="layer",
    )(
        tokens, glu_value, glu_gate, query_weight, key_weight, value_weight,
        norm_gain.reshape(1, D), gate_weight.T, gate_bias.reshape(1, 32), log_decay_extra.T, conv_taps,
        ln_gain.reshape(1, 256), ln_bias.reshape(1, 256), mem_gain.reshape(1, 256), out_conv, out_mem,
    )


VMEM_BYTES = 66700000
HOP1, SEED1, SIDE1 = 3.0, 6.1, 2.6
HOP2, SEED2, HOP3, SEED3, SIDE2 = 6.0, 10.0, 6.8, 11.0, 2.6
T2, TS, TY, TZ = 12.5, 27.5, 33.5, 42.0


def solution(mesh):
    split = Mesh(mesh.devices.reshape(NZ, NY, NX, 2), ("z", "y", "x", "c"))
    placed = (
        P(SP, TP), P(), P(SP, TP), P(SP, TP), P(None, TP), P(TP), P(TP), P(SP, TP), P(SP, TP), P(SP, TP),
        P(), P(), P(SP, None), P(TP), P(TP, None), P(TP, None),
    )
    return jax.shard_map(shards, mesh=split, in_specs=placed, out_specs=P(SP + TP, None), check_vma=False)
```
